256 devices in a mesh: grp: 2 (over y), ep: 32 (over z, core), tp: 4 (over x).
Axes of the slice: x: 4, y: 2, z: 16, core: 2. Of those that a mesh axis runs over, the one named last changes fastest.
The devices are a block of a 4x16x16 slice.
Arguments:
- mixer_tokens: bfloat16 [32768, 2048], P(('grp', 'ep', 'tp')), parts along dimension 0, may hold values from -6 to 6
- mixer_gain: bfloat16 [2048], replicated, may hold values from 0.099609375 to 1.8984375
- in_weight: bfloat16 [2048, 2048], P(None, 'tp'), may hold values from -0.125 to 0.125
- group_weight: bfloat16 [4, 512, 512], P('tp'), may hold values from -0.25 to 0.25
- channel_scale: bfloat16 [2048], P('tp'), may hold values from 0.099609375 to 1.8984375
- out_weight: bfloat16 [2048, 2048], P('tp'), may hold values from -0.125 to 0.125
- expert_tokens: bfloat16 [32768, 2048], P(('grp', 'ep', 'tp')), parts along dimension 0, may hold values from -6 to 6
- expert_gain: bfloat16 [2048], replicated, may hold values from 0.099609375 to 1.8984375
- route_ids: int32 [32768, 2], P(('grp', 'ep', 'tp')), parts along dimension 0, may hold values from 0 to 31, all different within a row; in each aligned block of 128 rows (0 to 127, 128 to 255, ...) at most 16 rows name the same one
- route_weights: float32 [32768, 2], P(('grp', 'ep', 'tp')), parts along dimension 0, may hold values from 0.1 to 1
- gate_weight: bfloat16 [32, 2048, 1024], P('ep', None, 'tp'), may hold values from -0.125 to 0.125
- up_weight: bfloat16 [32, 2048, 1024], P('ep', None, 'tp'), may hold values from -0.125 to 0.125
- down_weight: bfloat16 [32, 1024, 2048], P('ep', 'tp'), may hold values from -0.1875 to 0.1875
Outputs:
- mixed_tokens: bfloat16 [32768, 2048], P(('grp', 'ep', 'tp')), parts along dimension 0
- expert_mix: bfloat16 [32768, 2048], P(('grp', 'ep', 'tp')), parts along dimension 0
The draws below stay inside these ranges and needn't reach their ends.
There are 2 independent parts, one for each index of `grp`. The reference program is written for one: setup_inputs(seed, part) draws one part's arguments, and reference() takes and returns one part's arrays. A program takes and returns all parts, laid end to end along the dimension named above; an argument that names none is the same for every part. Nothing has to cross between parts.
Inputs may be any that keep to these rules, and one draw needn't show every extreme that they name: `route_ids`: each row names 2 different experts; in the rows of one device no expert is named more than 16 times, and one expert exactly 16 times in the rows of some device.
All inputs are finite; a program needn't handle non-finite values.
Results may differ from the reference program's by a relative error of at most 0.015.
Values may be sent and summed in bfloat16 or wider, within the bound.
A program may use at most 128 MiB of HBM per device.

```python
import math
import jax
import jax.numpy as jnp
import numpy as np
from jax import lax

D = 2048
GROUPS = 4
GW = 512
FF = 1024
FF_DEV = 256
TOP = 2
TOK_DEV = 128
TOKENS = 16384
EXPERTS = 32
CAP = 16
N_EP = 32
N_TP = 4


def block_levels(key, dims, split, least, high):
    def one(position, shards_of):
        heights = jax.random.uniform(jax.random.fold_in(jax.random.fold_in(key, 6), position), (shards_of,), jnp.float32, least / len(split), high / len(split))
        return jnp.repeat(jnp.exp(heights), dims[position] // shards_of).reshape((-1,) + (1,) * (len(dims) - position - 1))

    level = one(*split[0])
    for cut in split[1:]:
        level = level * one(*cut)
    return level


def routed_block(own_key, own, number, rows, number_of, top, bound, lean):
    order = jax.random.permutation(own_key, number_of)
    heavy_load, ordinary = portions_of(number_of, rows * top, bound, lean, True), portions_of(number_of, rows * top, bound, lean, False)
    places = jnp.arange(number_of)

    def named(lengths, rotation):
        used = int((lengths > 0).sum())
        fixed = max(1, used // 4)
        moved = fixed + (places - fixed + rotation * (used - fixed)) % max(1, number_of - fixed)
        return jnp.zeros((number_of,), jnp.int32).at[order[jnp.where(places < fixed, places, moved)]].set(jnp.asarray(lengths, jnp.int32))

    lengths = jnp.where(number % 4 == 0, named(heavy_load, number // 4), named(ordinary, number - number // 4 - 1))
    mixed = jax.random.permutation(jax.random.fold_in(own, 3), number_of)
    source_of, taker = mixed[0:number_of // 2 * 2:2], mixed[1:number_of // 2 * 2:2]
    room = jnp.minimum(lengths[source_of] - 1, bound - lengths[taker]) // 2
    room = jnp.where((source_of == order[0]) | (taker == order[0]) | (lengths[taker] == 0), 0, jnp.maximum(room, 0))
    moved = jax.random.randint(jax.random.fold_in(own, 4), (number_of // 2,), 0, 1 << 20) % (room + 1)
    lengths = lengths.at[source_of].add(-moved).at[taker].add(moved)
    labels = jnp.searchsorted(jnp.cumsum(lengths), jnp.arange(rows * top), side="right").astype(jnp.int32)
    listing = labels.reshape(top, rows).T
    listing = listing[jax.random.permutation(jax.random.fold_in(own, 1), rows)]
    rotation = jax.random.randint(jax.random.fold_in(own, 2), (rows, 1), 0, top)
    return jnp.take_along_axis(listing, (jnp.arange(top)[None, :] + rotation) % top, axis=1)


def portions_of(number_of, total, most, lean, full):
    loads = [(1 << 20) // math.isqrt(rank ** lean) + 1 for rank in range(1, number_of + 1)]
    largest = most if full else min(most, max(-(-total // number_of), total * loads[0] // sum(loads)))
    least = 1 if total - largest >= number_of - 1 else 0
    holding, spare = [largest] + [least] * (number_of - 1), total - largest - least * (number_of - 1)
    while spare > 0:
        free = [i for i in range(1, number_of) if holding[i] < largest] or [i for i in range(1, number_of) if holding[i] < most]
        pool, budget = sum([loads[i] for i in free]), spare
        for i in free:
            more = min(most - holding[i], max(1, budget * loads[i] // pool), spare)
            holding[i] = holding[i] + more
            spare = spare - more
    return np.array(holding)


def bell_draw(key, shape, scale, bound, split=(), kind=jnp.bfloat16):
    entries = jax.random.normal(key, shape, jnp.float32) * scale
    if len(split) > 0:
        entries = block_levels(key, shape, split, -0.22, 0.18) * entries
    return jnp.clip(entries, min=-bound, max=bound).astype(kind)


def setup_inputs(seed: int = 0, part: int = 0) -> dict:
    splits = jax.random.split(jax.random.key(seed), 14)
    part_keys = jax.random.split(jax.random.fold_in(splits[13], part), 14)
    mixer_tokens = bell_draw(part_keys[0], (TOKENS, D), 1.0, 6.0, ((0, 128),))
    mixer_gain = jnp.clip(1.0 + 0.18 * jax.random.normal(splits[1], (D,), jnp.float32), 0.099609375, 1.8984375).astype(jnp.bfloat16)
    in_weight = bell_draw(splits[2], (D, D), D ** -0.5, 0.125, ((1, 4),))
    group_weight = bell_draw(splits[3], (GROUPS, GW, GW), GW ** -0.5, 0.25, ((0, 4),))
    channel_scale = jnp.clip(1.0 + 0.18 * jax.random.normal(splits[4], (D,), jnp.float32), 0.099609375, 1.8984375).astype(jnp.bfloat16)
    out_weight = bell_draw(splits[5], (D, D), D ** -0.5, 0.125, ((0, 4),))
    expert_tokens = bell_draw(part_keys[6], (TOKENS, D), 1.0, 6.0, ((0, 128),))
    expert_gain = jnp.clip(1.0 + 0.18 * jax.random.normal(splits[7], (D,), jnp.float32), 0.099609375, 1.8984375).astype(jnp.bfloat16)
    route_ids_keys = jax.random.split(jax.random.fold_in(part_keys[8], 1), TOKENS // TOK_DEV)
    route_ids_turns = jax.random.permutation(jax.random.fold_in(part_keys[8], 3), TOKENS // TOK_DEV)
    route_ids = jax.vmap(lambda own, number: routed_block(jax.random.fold_in(part_keys[8], 2), own, number, TOK_DEV, EXPERTS, TOP, CAP, 2))(route_ids_keys, route_ids_turns).reshape((TOKENS, TOP))
    route_weights = jnp.clip(jnp.exp(math.log(1.0) - 2.3025851 * jax.random.uniform(part_keys[9], (TOKENS, TOP), jnp.float32) ** block_levels(part_keys[9], (TOKENS, TOP), ((0, 128),), -0.2, 0.2)), 0.1, 1.0)
    gate_weight = bell_draw(splits[10], (EXPERTS, D, FF), D ** -0.5, 0.125, ((0, 32), (2, 4)))
    up_weight = bell_draw(splits[11], (EXPERTS, D, FF), D ** -0.5, 0.125, ((0, 32), (2, 4)))
    down_weight = bell_draw(splits[12], (EXPERTS, FF, D), FF ** -0.5, 0.1875, ((0, 32), (1, 4)))
    return dict(mixer_tokens=mixer_tokens, mixer_gain=mixer_gain, in_weight=in_weight, group_weight=group_weight, channel_scale=channel_scale, out_weight=out_weight, expert_tokens=expert_tokens, expert_gain=expert_gain, route_ids=route_ids, route_weights=route_weights, gate_weight=gate_weight, up_weight=up_weight, down_weight=down_weight)


def rms_rows(rows, gain):
    values = rows.astype(jnp.float32)
    scaled = values * lax.rsqrt(lax.optimization_barrier(jnp.mean(values * values, axis=-1, keepdims=True)) + 1e-06)
    return (scaled * gain.astype(jnp.float32)).astype(jnp.bfloat16)

def expert_hidden(rows, w_gate, w_up):
    gate = jnp.dot(rows, w_gate, preferred_element_type=jnp.float32)
    upper = jnp.dot(rows, w_up, preferred_element_type=jnp.float32)
    return (jax.nn.silu(gate) * upper).astype(jnp.bfloat16)

def reference(mixer_tokens, mixer_gain, in_weight, group_weight, channel_scale, out_weight, expert_tokens, expert_gain, route_ids, route_weights, gate_weight, up_weight, down_weight):
    normed = rms_rows(mixer_tokens, mixer_gain)
    pooled_in = jnp.dot(normed, in_weight, preferred_element_type=jnp.float32).astype(jnp.bfloat16)
    values = pooled_in.astype(jnp.float32)
    length = values.shape[0]
    prefix = jnp.concatenate([jnp.zeros((1, D), jnp.float32), jnp.cumsum(values, axis=0)], axis=0)
    mixed = jnp.zeros((length, D), jnp.float32)
    for group in range(GROUPS):
        window = 2 ** (group + 1)
        low_col = group * GW
        upper = prefix[1:, low_col:low_col + GW]
        lower = jnp.concatenate([jnp.zeros((window - 1, GW), jnp.float32), prefix[:length - window + 1, low_col:low_col + GW]], axis=0)
        counts = jnp.minimum(jnp.arange(1, length + 1), window).astype(jnp.float32)
        trail = ((upper - lower) / counts[:, None] - values[:, low_col:low_col + GW]).astype(jnp.bfloat16)
        grouped = (jnp.dot(trail, group_weight[group], preferred_element_type=jnp.float32) * channel_scale[low_col:low_col + GW].astype(jnp.float32)).astype(jnp.bfloat16)
        partial_value = jnp.dot(grouped, out_weight[low_col:low_col + GW, :], preferred_element_type=jnp.float32)
        partial_value = lax.optimization_barrier(partial_value.astype(jnp.bfloat16))
        mixed = mixed + partial_value.astype(jnp.float32)
    mixed_tokens = mixed.astype(jnp.bfloat16)
    expert_in = rms_rows(expert_tokens, expert_gain)
    weights = route_weights.astype(jnp.float32)
    shares = weights / lax.optimization_barrier(jnp.sum(weights, axis=1, keepdims=True))
    count_tok = expert_in.shape[0]
    flat_ids = route_ids.reshape(count_tok * TOP).astype(jnp.int32)
    flat_tokens = jnp.concatenate([(jnp.arange(count_tok * TOP) // TOP).astype(jnp.int32), jnp.full((1,), count_tok, jnp.int32)])
    flat_shares = jnp.concatenate([shares.reshape(count_tok * TOP), jnp.zeros((1,), jnp.float32)])
    padded = jnp.concatenate([expert_in, jnp.zeros((1, D), jnp.bfloat16)], axis=0)
    most = N_EP * N_TP * CAP

    def one_expert(total, expert):
        chosen = jnp.nonzero(flat_ids == expert, size=most, fill_value=count_tok * TOP)[0].astype(jnp.int32)
        token_of = flat_tokens[chosen]
        rows = padded[token_of]
        hidden = expert_hidden(rows, gate_weight[expert], up_weight[expert])
        result = jnp.zeros((most, D), jnp.float32)
        for block in range(N_TP):
            part = jnp.dot(hidden[:, block * FF_DEV:(block + 1) * FF_DEV], down_weight[expert][block * FF_DEV:(block + 1) * FF_DEV, :], preferred_element_type=jnp.float32)
            part = lax.optimization_barrier(part.astype(jnp.bfloat16))
            result = result + part.astype(jnp.float32)
        total = total.at[token_of].add(result * flat_shares[chosen][:, None])
        return (total, None)
    total, _ = lax.scan(one_expert, jnp.zeros((count_tok + 1, D), jnp.float32), jnp.arange(EXPERTS).astype(jnp.int32))
    expert_mix = total[:count_tok].astype(jnp.bfloat16)
    return (mixed_tokens, expert_mix)
```

```python
import functools

import jax
import jax.numpy as jnp
from jax import lax
from jax.experimental import pallas as pl
from jax.experimental.pallas import tpu as pltpu
from jax.sharding import PartitionSpec as P

MESH = pl.DeviceIdType.MESH
F32 = jnp.float32
BF16 = jnp.bfloat16
WINDOW_MAX = 16


def dot(a, b):
    return jnp.dot(a, b, preferred_element_type=F32)


def rms_rows(rows, gain):
    values = rows.astype(F32)
    scaled = values * lax.rsqrt(jnp.mean(values * values, axis=-1, keepdims=True) + 1e-06)
    return (scaled * gain.astype(F32)).astype(BF16)


def far_first(j, n):
    return n // 2 + (1 - 2 * (j % 2)) * ((j + 1) // 2)


def kernel(
    n_ep, n_tp, cap,
    mtok, mgain, inw, gw, scale, ow, etok, egain, ids, ids_t, shares, gate, up, down,
    mixed_out, expert_out,
    xin, out_buf, in_buf, res_buf, ret_buf, acc, wg, wu, wd,
    mrows, normed, inw_v, gw_v, ow_v, ext, part_buf, part_in, mixed_v, expert_v,
    load_sem, tok_send, tok_recv, ret_send, ret_recv, w_send, w_recv,
    ag_send, ag_recv, halo_send, halo_recv, rs_send, rs_recv, out_sem,
):
    ep = lax.axis_index("ep")
    tp = lax.axis_index("tp")
    rows, width = etok.shape
    n_slots = n_ep * cap
    half = n_ep // 2
    right, left = (tp + 1) % n_tp, (tp + n_tp - 1) % n_tp
    depth = down.shape[1]

    barrier = pltpu.get_barrier_semaphore()

    @pl.loop(1, n_ep)
    def _(r):
        pl.semaphore_signal(
            barrier, inc=1, device_id={"ep": (ep + r) % n_ep}, device_id_type=MESH
        )

    for r in range(1, n_tp):
        pl.semaphore_signal(
            barrier, inc=1, device_id={"tp": (tp + r) % n_tp}, device_id_type=MESH
        )

    loads = [
        pltpu.make_async_copy(src, dst, load_sem.at[i])
        for i, (src, dst) in enumerate(
            [
                (gate.at[0], wg.at[0]),
                (up.at[0], wu.at[0]),
                (down.at[0], wd.at[0]),
                (mtok, mrows),
                (inw, inw_v),
                (gw.at[0], gw_v),
                (ow, ow_v),
            ]
        )
    ]
    for load in loads:
        load.start()

    def weights(i, src, dst, to):
        return pltpu.make_async_remote_copy(
            src_ref=src,
            dst_ref=dst,
            send_sem=w_send.at[i],
            recv_sem=w_recv.at[i],
            device_id={"tp": to},
            device_id_type=MESH,
        )

    low, high = pl.ds(0, depth // 2), pl.ds(depth // 2, depth // 2)
    to_right = [
        weights(0, gate.at[0], wg.at[1], right),
        weights(1, down.at[0], wd.at[1], right),
        weights(2, up.at[0], wu.at[1], right),
    ]
    to_left = [
        weights(3, up.at[0], wu.at[2], left),
        weights(4, down.at[0], wd.at[2], left),
        weights(5, gate.at[0], wg.at[2], left),
    ]
    on_right = [
        weights(6, wg.at[1], wg.at[3], right),
        weights(7, wd.at[1, low], wd.at[3, low], right),
    ]
    on_left = [
        weights(8, wu.at[2], wu.at[3], left),
        weights(9, wd.at[2, high], wd.at[3, high], left),
    ]

    xin[...] = rms_rows(etok[...], egain[...])
    experts = lax.broadcasted_iota(jnp.int32, (n_ep, rows), 0)
    firsts = [ids_t[k : k + 1, :] == experts for k in range(2)]
    named = jnp.where(firsts[0] | firsts[1], 1.0, 0.0).astype(BF16)
    earlier = jnp.where(
        lax.broadcasted_iota(jnp.int32, (rows, rows), 0)
        < lax.broadcasted_iota(jnp.int32, (rows, rows), 1),
        1.0,
        0.0,
    ).astype(BF16)
    before = dot(named, earlier)
    targets_t = [
        ids_t[k : k + 1, :] * cap
        + jnp.sum(jnp.where(firsts[k], before, 0.0), axis=0, keepdims=True).astype(jnp.int32)
        for k in range(2)
    ]
    group = min(8, n_ep)

    @pl.loop(0, n_ep // group)
    def _(q):
        slots = lax.broadcasted_iota(jnp.int32, (group * cap, rows), 0) + q * group * cap
        place = jnp.where((slots == targets_t[0]) | (slots == targets_t[1]), 1.0, 0.0).astype(BF16)
        out_buf[pl.ds(q * group, group)] = (
            dot(place, xin[...]).astype(BF16).reshape(group, cap, width)
        )

    in_buf[n_ep - 1] = out_buf[ep]

    pl.semaphore_wait(barrier, n_ep - 1 + n_tp - 1)

    for a, b in zip(to_right, to_left):
        a.start()
        b.start()

    def token_copy(j):
        to = (ep + far_first(j, n_ep)) % n_ep
        return pltpu.make_async_remote_copy(
            src_ref=out_buf.at[to],
            dst_ref=in_buf.at[j],
            send_sem=tok_send.at[j],
            recv_sem=tok_recv.at[j],
            device_id={"ep": to},
            device_id_type=MESH,
        )

    @pl.loop(0, n_ep - 1)
    def _(j):
        token_copy(j).start()

    loads[3].wait()
    normed[tp] = rms_rows(mrows[...], mgain[...])

    acc[...] = jnp.zeros_like(acc)
    to_right[0].wait_recv()
    on_right[0].start()
    to_left[0].wait_recv()
    on_left[0].start()
    to_right[1].wait_recv()
    on_right[1].start()
    to_left[1].wait_recv()
    on_left[1].start()

    def spread(r):
        return pltpu.make_async_remote_copy(
            src_ref=normed.at[tp],
            dst_ref=normed.at[tp],
            send_sem=ag_send.at[r],
            recv_sem=ag_recv.at[r],
            device_id={"tp": (tp + r) % n_tp},
            device_id_type=MESH,
        )

    for r in (2, 1, 3):
        spread(r).start()

    for i in range(3):
        loads[i].wait()

    @pl.loop(0, n_ep - 1)
    def _(j):
        token_copy(j).wait_recv()

    tiles = 2
    per_tile = n_ep // tiles
    tile_rows = per_tile * cap
    step = min(512, width)

    def serve(s, m, last):
        x = in_buf[pl.ds(m * per_tile, per_tile)].reshape(tile_rows, width)
        g = dot(x, wg[s])
        u = dot(x, wu[s])
        hidden = (g / (1.0 + jnp.exp(-g)) * u).astype(BF16)
        for c in range(0, width, step):
            part = dot(hidden, wd[s, :, c : c + step]).astype(BF16).astype(F32)
            total = acc[m, :, c : c + step] + part
            if last:
                res_buf[pl.ds(m * per_tile, per_tile), :, c : c + step] = total.astype(BF16).reshape(
                    per_tile, cap, step
                )
            else:
                acc[m, :, c : c + step] = total

    def serve_all(s):
        @pl.loop(0, tiles)
        def _(m):
            serve(s, m, False)

    serve_all(0)
    to_right[2].wait_recv()
    serve_all(1)
    to_left[2].wait_recv()
    serve_all(2)
    for copy in (*on_right, *on_left):
        copy.wait_recv()

    def result_copy(j):
        to = (ep + n_ep - far_first(j, n_ep)) % n_ep
        return pltpu.make_async_remote_copy(
            src_ref=res_buf.at[j],
            dst_ref=ret_buf.at[ep],
            send_sem=ret_send.at[j],
            recv_sem=ret_recv.at[j],
            device_id={"ep": to},
            device_id_type=MESH,
        )

    @pl.loop(0, tiles)
    def _(m):
        serve(3, m, True)

        @pl.loop(m * per_tile, jnp.minimum((m + 1) * per_tile, n_ep - 1))
        def _(j):
            result_copy(j).start()

    ret_buf[ep] = res_buf[n_ep - 1]

    for i in range(4, 7):
        loads[i].wait()
    ext[0] = jnp.zeros((rows, ext.shape[2]), BF16)
    ext[tp + 1] = dot(normed[tp], inw_v[...]).astype(BF16)
    for r in (1, 3, 2):
        spread(r).wait_recv()
        src = (tp + n_tp - r) % n_tp
        ext[src + 1] = dot(normed[src], inw_v[...]).astype(BF16)
    edge = pl.ds(rows - WINDOW_MAX, WINDOW_MAX)
    halo = pltpu.make_async_remote_copy(
        src_ref=ext.at[n_tp, edge],
        dst_ref=ext.at[n_tp + 1, pl.ds(0, WINDOW_MAX)],
        send_sem=halo_send,
        recv_sem=halo_recv,
        device_id={"ep": (ep + 1) % n_ep},
        device_id_type=MESH,
    )
    halo.start()
    window = jnp.left_shift(jnp.int32(2), tp)
    lag = lax.broadcasted_iota(jnp.int32, (rows, rows), 0) - lax.broadcasted_iota(
        jnp.int32, (rows, rows), 1
    )
    band = jnp.where((lag >= 0) & (lag < window), 1.0, 0.0).astype(BF16)
    band_before = jnp.where(lag + rows < window, 1.0, 0.0).astype(BF16)
    place_in = lax.broadcasted_iota(jnp.int32, (rows, 1), 0) + 1
    halo.wait_recv()
    ext[0, edge, :] = jnp.where(ep == 0, 0.0, ext[n_tp + 1, 0:WINDOW_MAX, :].astype(F32)).astype(BF16)

    def sums(r):
        to = (tp + r) % n_tp
        return pltpu.make_async_remote_copy(
            src_ref=part_buf.at[to],
            dst_ref=part_in.at[r - 1],
            send_sem=rs_send.at[r],
            recv_sem=rs_recv.at[r],
            device_id={"tp": to},
            device_id_type=MESH,
        )

    for r in (2, 1, 3, 0):
        m = (tp + r) % n_tp
        here = ext[m + 1]
        total = dot(band, here) + dot(band_before, ext[m])
        counts = jnp.minimum(place_in + (ep * n_tp + m) * rows, window).astype(F32)
        pooled = (total / counts - here.astype(F32)).astype(BF16)
        grouped = (dot(pooled, gw_v[...]) * scale[...].astype(F32)).astype(BF16)
        for c in range(0, width, step):
            part_buf[m, :, c : c + step] = dot(grouped, ow_v[:, c : c + step]).astype(BF16)
        if r:
            sums(r).start()

    for r in (1, 3, 2):
        sums(r).wait_recv()
    total = part_buf[tp].astype(F32)
    for r in range(n_tp - 1):
        total = total + part_in[r].astype(F32)
    mixed_v[...] = total.astype(BF16)
    mixed_store = pltpu.make_async_copy(mixed_v, mixed_out, out_sem.at[0])
    mixed_store.start()

    lanes = lax.broadcasted_iota(jnp.int32, (rows, n_ep), 1)
    mine = [ids[:, k : k + 1] == lanes for k in range(2)]
    named_rows = jnp.where(mine[0] | mine[1], 1.0, 0.0).astype(BF16)
    later = jnp.where(lag > 0, 1.0, 0.0).astype(BF16)
    before_rows = dot(later, named_rows)
    slots = lax.broadcasted_iota(jnp.int32, (rows, n_slots), 1)
    picks = []
    for k in range(2):
        target = ids[:, k : k + 1] * cap + jnp.sum(
            jnp.where(mine[k], before_rows, 0.0), axis=1, keepdims=True
        ).astype(jnp.int32)
        picks.append(jnp.where(slots == target, 1.0, 0.0).astype(BF16))
    weight = shares[...]
    weight = weight / jnp.sum(weight, axis=1, keepdims=True)

    @pl.loop(0, n_ep - 1)
    def _(j):
        result_copy(j).wait_recv()

    for c in range(0, width, step):
        back = ret_buf[:, :, c : c + step].reshape(n_slots, step)
        mix = dot(picks[0], back) * weight[:, 0:1] + dot(picks[1], back) * weight[:, 1:2]
        expert_v[:, c : c + step] = mix.astype(BF16)
    expert_store = pltpu.make_async_copy(expert_v, expert_out, out_sem.at[1])
    expert_store.start()

    for copy in (*to_right, *to_left, *on_right, *on_left):
        copy.wait_send()

    @pl.loop(0, n_ep - 1)
    def _(j):
        token_copy(j).wait_send()
        result_copy(j).wait_send()

    for r in range(1, n_tp):
        spread(r).wait_send()
        sums(r).wait_send()
    halo.wait_send()
    mixed_store.wait()
    expert_store.wait()


def solution(mesh):
    n_ep, n_tp = mesh.shape["ep"], mesh.shape["tp"]

    def local(
        mixer_tokens, mixer_gain, in_weight, group_weight, channel_scale, out_weight,
        expert_tokens, expert_gain, route_ids, route_weights, gate_weight, up_weight, down_weight,
    ):
        rows, width = expert_tokens.shape
        cap = 4 * rows // n_ep
        gw = in_weight.shape[1]
        ff = gate_weight.shape[2]
        vmem = pl.BlockSpec(memory_space=pltpu.VMEM)
        hbm = pl.BlockSpec(memory_space=pl.ANY)
        slots = n_ep * cap
        V = pltpu.VMEM
        dma = pltpu.SemaphoreType.DMA
        out = jax.ShapeDtypeStruct((rows, width), BF16)
        return pl.pallas_call(
            functools.partial(kernel, n_ep, n_tp, cap),
            out_shape=(out, out),
            in_specs=[hbm, vmem, hbm, hbm, vmem, hbm, vmem, vmem, vmem, vmem, vmem, hbm, hbm, hbm],
            out_specs=(hbm, hbm),
            scratch_shapes=[
                V((rows, width), BF16),
                V((n_ep, cap, width), BF16),
                V((n_ep, cap, width), BF16),
                V((n_ep, cap, width), BF16),
                V((n_ep, cap, width), BF16),
                V((2, slots // 2, width), F32),
                V((n_tp, width, ff), BF16),
                V((n_tp, width, ff), BF16),
                V((n_tp, ff, width), BF16),
                V((rows, width), BF16),
                V((n_tp, rows, width), BF16),
                V((width, gw), BF16),
                V((gw, gw), BF16),
                V((gw, width), BF16),
                V((n_tp + 2, rows, gw), BF16),
                V((n_tp, rows, width), BF16),
                V((n_tp - 1, rows, width), BF16),
                V((rows, width), BF16),
                V((rows, width), BF16),
                dma((7,)),
                dma((n_ep - 1,)),
                dma((n_ep - 1,)),
                dma((n_ep - 1,)),
                dma((n_ep - 1,)),
                dma((10,)),
                dma((10,)),
                dma((n_tp,)),
                dma((n_tp,)),
                dma,
                dma,
                dma((n_tp,)),
                dma((n_tp,)),
                dma((2,)),
            ],
            compiler_params=pltpu.CompilerParams(
                collective_id=0, has_side_effects=True, vmem_limit_bytes=58 * 1024 * 1024
            ),
        )(
            mixer_tokens, mixer_gain[None], in_weight, group_weight, channel_scale[None], out_weight,
            expert_tokens, expert_gain[None], route_ids, route_ids.T, route_weights,
            gate_weight, up_weight, down_weight,
        )

    block = P(("grp", "ep", "tp"), None)
    placed = (
        block, P(), P(None, "tp"), P("tp", None, None), P("tp"), P("tp", None),
        block, P(), block, block, P("ep", None, "tp"), P("ep", None, "tp"), P("ep", "tp", None),
    )
    return jax.shard_map(
        local, mesh=mesh, in_specs=placed, out_specs=(block, block), check_vma=False
    )
```

```python
import functools

import jax
import jax.numpy as jnp
from jax import lax
from jax.experimental import pallas as pl
from jax.experimental.pallas import tpu as pltpu
from jax.sharding import PartitionSpec as P

MESH = pl.DeviceIdType.MESH
F32 = jnp.float32
BF16 = jnp.bfloat16
WINDOW_MAX = 16


def dot(a, b):
    return jnp.dot(a, b, preferred_element_type=F32)


def rms_rows(rows, gain):
    values = rows.astype(F32)
    scaled = values * lax.rsqrt(jnp.mean(values * values, axis=-1, keepdims=True) + 1e-06)
    return (scaled * gain.astype(F32)[None]).astype(BF16)


def far_first(j, n):
    return n // 2 + (1 - 2 * (j % 2)) * ((j + 1) // 2)


def kernel(
    n_ep, n_tp, cap,
    mtok, mgain_h, inw, gw, scale_h, ow, etok_h, egain_h, ids_h, shares_h, gate, up, down,
    mixed_out, expert_out,
    etok, egain, mgain, scale, ids_t, shares_t,
    xin, out_buf, in_buf, res_buf, ret_buf, acc, wg, wu, wd,
    mrows, normed, tail, edge_out, edge_in, inw_v, gw_v, ow_v, ext, part_buf, part_in,
    load_sem, tok_send, tok_recv, ret_send, ret_recv, w_send, w_recv,
    ag_send, ag_recv, tail_send, tail_recv, halo_send, halo_recv, rs_send, rs_recv,
):
    ep = lax.axis_index("ep")
    tp = lax.axis_index("tp")
    rows, width = mtok.shape
    n_slots = n_ep * cap
    half = n_ep // 2
    right, left = (tp + 1) % n_tp, (tp + n_tp - 1) % n_tp
    depth = down.shape[1]

    barrier = pltpu.get_barrier_semaphore()

    @pl.loop(1, n_ep)
    def _(r):
        pl.semaphore_signal(
            barrier, inc=1, device_id={"ep": (ep + r) % n_ep}, device_id_type=MESH
        )

    for r in range(1, n_tp):
        pl.semaphore_signal(
            barrier, inc=1, device_id={"tp": (tp + r) % n_tp}, device_id_type=MESH
        )

    loads = [
        pltpu.make_async_copy(src, dst, load_sem.at[i])
        for i, (src, dst) in enumerate(
            [
                (etok_h, etok),
                (egain_h, egain),
                (ids_h, ids_t),
                (shares_h, shares_t),
                (mgain_h, mgain),
                (scale_h, scale),
                (mtok, mrows),
                (inw, inw_v),
                (gate.at[0], wg.at[0]),
                (up.at[0], wu.at[0]),
                (down.at[0], wd.at[0]),
                (gw.at[0], gw_v),
                (ow, ow_v),
            ]
        )
    ]
    for load in loads:
        load.start()
    for i in range(3):
        loads[i].wait()

    def weights(i, src, dst, to):
        return pltpu.make_async_remote_copy(
            src_ref=src,
            dst_ref=dst,
            send_sem=w_send.at[i],
            recv_sem=w_recv.at[i],
            device_id={"tp": to},
            device_id_type=MESH,
        )

    low, high = pl.ds(0, depth // 2), pl.ds(depth // 2, depth // 2)
    to_right = [
        weights(0, gate.at[0], wg.at[1], right),
        weights(1, down.at[0], wd.at[1], right),
        weights(2, up.at[0], wu.at[1], right),
    ]
    to_left = [
        weights(3, up.at[0], wu.at[2], left),
        weights(4, down.at[0], wd.at[2], left),
        weights(5, gate.at[0], wg.at[2], left),
    ]
    on_right = [
        weights(6, wg.at[1], wg.at[3], right),
        weights(7, wd.at[1, low], wd.at[3, low], right),
    ]
    on_left = [
        weights(8, wu.at[2], wu.at[3], left),
        weights(9, wd.at[2, high], wd.at[3, high], left),
    ]

    xin[...] = rms_rows(etok[...], egain[...])
    experts = lax.broadcasted_iota(jnp.int32, (n_ep, rows), 0)
    firsts = [ids_t[k : k + 1, :] == experts for k in range(2)]
    named = jnp.where(firsts[0] | firsts[1], 1.0, 0.0).astype(BF16)
    earlier = jnp.where(
        lax.broadcasted_iota(jnp.int32, (rows, rows), 0)
        < lax.broadcasted_iota(jnp.int32, (rows, rows), 1),
        1.0,
        0.0,
    ).astype(BF16)
    before = dot(named, earlier)
    targets_t = [
        ids_t[k : k + 1, :] * cap
        + jnp.sum(jnp.where(firsts[k], before, 0.0), axis=0, keepdims=True).astype(jnp.int32)
        for k in range(2)
    ]
    group = min(8, n_ep)

    @pl.loop(0, n_ep // group)
    def _(q):
        slots = lax.broadcasted_iota(jnp.int32, (group * cap, rows), 0) + q * group * cap
        place = jnp.where((slots == targets_t[0]) | (slots == targets_t[1]), 1.0, 0.0).astype(BF16)
        out_buf[pl.ds(q * group, group)] = (
            dot(place, xin[...]).astype(BF16).reshape(group, cap, width)
        )

    in_buf[n_ep - 1] = out_buf[ep]

    pl.semaphore_wait(barrier, n_ep - 1 + n_tp - 1)

    for a, b in zip(to_right, to_left):
        a.start()
        b.start()

    def token_copy(j):
        to = (ep + far_first(j, n_ep)) % n_ep
        return pltpu.make_async_remote_copy(
            src_ref=out_buf.at[to],
            dst_ref=in_buf.at[j],
            send_sem=tok_send.at[j],
            recv_sem=tok_recv.at[j],
            device_id={"ep": to},
            device_id_type=MESH,
        )

    @pl.loop(0, n_ep - 1)
    def _(j):
        token_copy(j).start()

    loads[4].wait()
    loads[6].wait()
    normed[tp] = rms_rows(mrows[...], mgain[...])

    edge = pl.ds(rows - WINDOW_MAX, WINDOW_MAX)

    def tail_copy(r):
        return pltpu.make_async_remote_copy(
            src_ref=normed.at[n_tp - 1, edge],
            dst_ref=tail,
            send_sem=tail_send.at[r],
            recv_sem=tail_recv,
            device_id={"tp": (tp + r) % n_tp},
            device_id_type=MESH,
        )

    loads[7].wait()

    @pl.when(tp == n_tp - 1)
    def _():
        for r in (2, 1, 3):
            tail_copy(r).start()
        tail[...] = normed[n_tp - 1, edge]

    @pl.when(tp != n_tp - 1)
    def _():
        tail_copy(0).wait_recv()

    edge_out[...] = dot(tail[...], inw_v[...]).astype(BF16)
    halo = pltpu.make_async_remote_copy(
        src_ref=edge_out,
        dst_ref=edge_in,
        send_sem=halo_send,
        recv_sem=halo_recv,
        device_id={"ep": (ep + 1) % n_ep},
        device_id_type=MESH,
    )
    halo.start()

    acc[...] = jnp.zeros_like(acc)
    to_right[0].wait_recv()
    on_right[0].start()
    to_left[0].wait_recv()
    on_left[0].start()
    to_right[1].wait_recv()
    on_right[1].start()
    to_left[1].wait_recv()
    on_left[1].start()

    def spread(r):
        return pltpu.make_async_remote_copy(
            src_ref=normed.at[tp],
            dst_ref=normed.at[tp],
            send_sem=ag_send.at[r],
            recv_sem=ag_recv.at[r],
            device_id={"tp": (tp + r) % n_tp},
            device_id_type=MESH,
        )

    for r in (2, 1, 3):
        spread(r).start()

    for i in range(8, 11):
        loads[i].wait()

    @pl.loop(0, n_ep - 1)
    def _(j):
        token_copy(j).wait_recv()

    tiles = 2
    per_tile = n_ep // tiles
    tile_rows = per_tile * cap
    step = min(512, width)

    def serve(s, m, last):
        x = in_buf[pl.ds(m * per_tile, per_tile)].reshape(tile_rows, width)
        g = dot(x, wg[s])
        u = dot(x, wu[s])
        hidden = (g / (1.0 + jnp.exp(-g)) * u).astype(BF16)
        for c in range(0, width, step):
            part = dot(hidden, wd[s, :, c : c + step]).astype(BF16).astype(F32)
            total = acc[m, :, c : c + step] + part
            if last:
                res_buf[pl.ds(m * per_tile, per_tile), :, c : c + step] = total.astype(BF16).reshape(
                    per_tile, cap, step
                )
            else:
                acc[m, :, c : c + step] = total

    def serve_all(s):
        @pl.loop(0, tiles)
        def _(m):
            serve(s, m, False)

    serve_all(0)
    to_right[2].wait_recv()
    serve_all(1)
    to_left[2].wait_recv()
    serve_all(2)
    for copy in (*on_right, *on_left):
        copy.wait_recv()

    def result_copy(j):
        to = (ep + n_ep - far_first(j, n_ep)) % n_ep
        return pltpu.make_async_remote_copy(
            src_ref=res_buf.at[j],
            dst_ref=ret_buf.at[ep],
            send_sem=ret_send.at[j],
            recv_sem=ret_recv.at[j],
            device_id={"ep": to},
            device_id_type=MESH,
        )

    @pl.loop(0, tiles)
    def _(m):
        serve(3, m, True)

        @pl.loop(m * per_tile, jnp.minimum((m + 1) * per_tile, n_ep - 1))
        def _(j):
            result_copy(j).start()

    ret_buf[ep] = res_buf[n_ep - 1]

    for i in (3, 5, 11, 12):
        loads[i].wait()
    ext[0] = jnp.zeros((rows, ext.shape[2]), BF16)
    ext[tp + 1] = dot(normed[tp], inw_v[...]).astype(BF16)
    for r in (1, 3, 2):
        spread(r).wait_recv()
        src = (tp + n_tp - r) % n_tp
        ext[src + 1] = dot(normed[src], inw_v[...]).astype(BF16)
    window = jnp.left_shift(jnp.int32(2), tp)
    lag = lax.broadcasted_iota(jnp.int32, (rows, rows), 0) - lax.broadcasted_iota(
        jnp.int32, (rows, rows), 1
    )
    band = jnp.where((lag >= 0) & (lag < window), 1.0, 0.0).astype(BF16)
    band_before = jnp.where(lag + rows < window, 1.0, 0.0).astype(BF16)
    place_in = lax.broadcasted_iota(jnp.int32, (rows, 1), 0) + 1
    halo.wait_recv()
    ext[0, edge, :] = jnp.where(ep == 0, 0.0, edge_in[...].astype(F32)).astype(BF16)

    def sums(r):
        to = (tp + r) % n_tp
        return pltpu.make_async_remote_copy(
            src_ref=part_buf.at[to],
            dst_ref=part_in.at[r - 1],
            send_sem=rs_send.at[r],
            recv_sem=rs_recv.at[r],
            device_id={"tp": to},
            device_id_type=MESH,
        )

    for r in (2, 1, 3, 0):
        m = (tp + r) % n_tp
        here = ext[m + 1]
        total = dot(band, here) + dot(band_before, ext[m])
        counts = jnp.minimum(place_in + (ep * n_tp + m) * rows, window).astype(F32)
        pooled = (total / counts - here.astype(F32)).astype(BF16)
        grouped = (dot(pooled, gw_v[...]) * scale[...].astype(F32)[None]).astype(BF16)
        for c in range(0, width, step):
            part_buf[m, :, c : c + step] = dot(grouped, ow_v[:, c : c + step]).astype(BF16)
        if r:
            sums(r).start()

    for r in (1, 3, 2):
        sums(r).wait_recv()
    total = part_buf[tp].astype(F32)
    for r in range(n_tp - 1):
        total = total + part_in[r].astype(F32)
    mixed_out[...] = total.astype(BF16)

    ids = jnp.transpose(ids_t[...])
    shares = jnp.transpose(shares_t[...])
    lanes = lax.broadcasted_iota(jnp.int32, (rows, n_ep), 1)
    mine = [ids[:, k : k + 1] == lanes for k in range(2)]
    named_rows = jnp.where(mine[0] | mine[1], 1.0, 0.0).astype(BF16)
    later = jnp.where(lag > 0, 1.0, 0.0).astype(BF16)
    before_rows = dot(later, named_rows)
    slots = lax.broadcasted_iota(jnp.int32, (rows, n_slots), 1)
    picks = []
    for k in range(2):
        target = ids[:, k : k + 1] * cap + jnp.sum(
            jnp.where(mine[k], before_rows, 0.0), axis=1, keepdims=True
        ).astype(jnp.int32)
        picks.append(jnp.where(slots == target, 1.0, 0.0).astype(BF16))
    weight = shares / jnp.sum(shares, axis=1, keepdims=True)

    @pl.loop(0, n_ep - 1)
    def _(j):
        result_copy(j).wait_recv()

    for c in range(0, width, step):
        back = ret_buf[:, :, c : c + step].reshape(n_slots, step)
        mix = dot(picks[0], back) * weight[:, 0:1] + dot(picks[1], back) * weight[:, 1:2]
        expert_out[:, c : c + step] = mix.astype(BF16)

    for copy in (*to_right, *to_left, *on_right, *on_left):
        copy.wait_send()

    @pl.loop(0, n_ep - 1)
    def _(j):
        token_copy(j).wait_send()
        result_copy(j).wait_send()

    for r in range(1, n_tp):
        spread(r).wait_send()
        sums(r).wait_send()
    halo.wait_send()

    @pl.when(tp == n_tp - 1)
    def _():
        for r in range(1, n_tp):
            tail_copy(r).wait_send()


def solution(mesh):
    n_ep, n_tp = mesh.shape["ep"], mesh.shape["tp"]

    def local(
        mixer_tokens, mixer_gain, in_weight, group_weight, channel_scale, out_weight,
        expert_tokens, expert_gain, route_ids, route_weights, gate_weight, up_weight, down_weight,
    ):
        rows, width = expert_tokens.shape
        cap = 4 * rows // n_ep
        gw = in_weight.shape[1]
        ff = gate_weight.shape[2]
        vmem = pl.BlockSpec(memory_space=pltpu.VMEM)
        hbm = pl.BlockSpec(memory_space=pl.ANY)
        slots = n_ep * cap
        V = pltpu.VMEM
        dma = pltpu.SemaphoreType.DMA
        out = jax.ShapeDtypeStruct((rows, width), BF16)
        return pl.pallas_call(
            functools.partial(kernel, n_ep, n_tp, cap),
            out_shape=(out, out),
            in_specs=[hbm] * 13,
            out_specs=(vmem, vmem),
            scratch_shapes=[
                V((rows, width), BF16),
                V((width,), BF16),
                V((width,), BF16),
                V((gw,), BF16),
                V((2, rows), jnp.int32),
                V((2, rows), F32),
                V((rows, width), BF16),
                V((n_ep, cap, width), BF16),
                V((n_ep, cap, width), BF16),
                V((n_ep, cap, width), BF16),
                V((n_ep, cap, width), BF16),
                V((2, slots // 2, width), F32),
                V((n_tp, width, ff), BF16),
                V((n_tp, width, ff), BF16),
                V((n_tp, ff, width), BF16),
                V((rows, width), BF16),
                V((n_tp, rows, width), BF16),
                V((WINDOW_MAX, width), BF16),
                V((WINDOW_MAX, gw), BF16),
                V((WINDOW_MAX, gw), BF16),
                V((width, gw), BF16),
                V((gw, gw), BF16),
                V((gw, width), BF16),
                V((n_tp + 1, rows, gw), BF16),
                V((n_tp, rows, width), BF16),
                V((n_tp - 1, rows, width), BF16),
                dma((13,)),
                dma((n_ep - 1,)),
                dma((n_ep - 1,)),
                dma((n_ep - 1,)),
                dma((n_ep - 1,)),
                dma((10,)),
                dma((10,)),
                dma((n_tp,)),
                dma((n_tp,)),
                dma((n_tp,)),
                dma,
                dma,
                dma,
                dma((n_tp,)),
                dma((n_tp,)),
            ],
            compiler_params=pltpu.CompilerParams(
                collective_id=0, has_side_effects=True, vmem_limit_bytes=52 * 1024 * 1024
            ),
        )(
            *(
                pltpu.with_memory_space_constraint(a, pltpu.HBM)
                for a in (
                    mixer_tokens, mixer_gain, in_weight, group_weight, channel_scale, out_weight,
                    expert_tokens, expert_gain, route_ids.T, route_weights.T,
                    gate_weight, up_weight, down_weight,
                )
            )
        )

    block = P(("grp", "ep", "tp"), None)
    placed = (
        block, P(), P(None, "tp"), P("tp", None, None), P("tp"), P("tp", None),
        block, P(), block, block, P("ep", None, "tp"), P("ep", None, "tp"), P("ep", "tp", None),
    )
    return jax.shard_map(
        local, mesh=mesh, in_specs=placed, out_specs=(block, block), check_vma=False
    )
```

```python
import functools

import jax
import jax.numpy as jnp
from jax import lax
from jax.experimental import pallas as pl
from jax.experimental.pallas import tpu as pltpu
from jax.sharding import PartitionSpec as P

MESH = pl.DeviceIdType.MESH
F32 = jnp.float32
BF16 = jnp.bfloat16
WINDOW_MAX = 16


def dot(a, b):
    return jnp.dot(a, b, preferred_element_type=F32)


def rms_rows(rows, gain):
    values = rows.astype(F32)
    scaled = values * lax.rsqrt(jnp.mean(values * values, axis=-1, keepdims=True) + 1e-06)
    return (scaled * gain.astype(F32)[None]).astype(BF16)


def far_first(j, n):
    return n // 2 + (1 - 2 * (j % 2)) * ((j + 1) // 2)


def kernel(
    n_ep, n_tp, cap,
    mtok, mgain_h, inw, gw, scale_h, ow, etok_h, egain_h, ids_h, shares_h, gate, up, down,
    mixed_out, expert_out,
    etok, egain, mgain, scale, ids_t, shares_t,
    xin, out_buf, in_buf, peer_buf, res_buf, ret_buf, acc, part_out, part_back, wg, wu, wd,
    mrows, normed, tail, edge_out, edge_in, inw_v, gw_v, ow_v, ext, part_buf, part_in,
    load_sem, tok_send, tok_recv, swap_send, swap_recv, back_send, back_recv,
    ret_send, ret_recv, w_send, w_recv,
    ag_send, ag_recv, tail_send, tail_recv, halo_send, halo_recv, rs_send, rs_recv,
):
    ep = lax.axis_index("ep")
    tp = lax.axis_index("tp")
    rows, width = mtok.shape
    n_slots = n_ep * cap
    n_z = n_ep // 2
    z, core = ep // 2, ep % 2

    barrier = pltpu.get_barrier_semaphore()

    @pl.loop(1, n_ep)
    def _(r):
        pl.semaphore_signal(
            barrier, inc=1, device_id={"ep": (ep + r) % n_ep}, device_id_type=MESH
        )

    for r in range(1, n_tp):
        pl.semaphore_signal(
            barrier, inc=1, device_id={"tp": (tp + r) % n_tp}, device_id_type=MESH
        )

    loads = [
        pltpu.make_async_copy(src, dst, load_sem.at[i])
        for i, (src, dst) in enumerate(
            [
                (etok_h, etok),
                (egain_h, egain),
                (ids_h, ids_t),
                (shares_h, shares_t),
                (mgain_h, mgain),
                (scale_h, scale),
                (mtok, mrows),
                (inw, inw_v),
                (gate.at[0], wg.at[0]),
                (up.at[0], wu.at[0]),
                (down.at[0], wd.at[0]),
                (gw.at[0], gw_v),
                (ow, ow_v),
            ]
        )
    ]
    for load in loads:
        load.start()
    for i in range(3):
        loads[i].wait()

    def weights(i, src, dst):
        return pltpu.make_async_remote_copy(
            src_ref=src,
            dst_ref=dst,
            send_sem=w_send.at[i],
            recv_sem=w_recv.at[i],
            device_id={"tp": tp + 1 - 2 * (tp % 2)},
            device_id_type=MESH,
        )

    shard_copies = [
        weights(0, gate.at[0], wg.at[1]),
        weights(1, up.at[0], wu.at[1]),
        weights(2, down.at[0], wd.at[1]),
    ]

    xin[...] = rms_rows(etok[...], egain[...])
    experts = lax.broadcasted_iota(jnp.int32, (n_ep, rows), 0)
    firsts = [ids_t[k : k + 1, :] == experts for k in range(2)]
    named = jnp.where(firsts[0] | firsts[1], 1.0, 0.0).astype(BF16)
    earlier = jnp.where(
        lax.broadcasted_iota(jnp.int32, (rows, rows), 0)
        < lax.broadcasted_iota(jnp.int32, (rows, rows), 1),
        1.0,
        0.0,
    ).astype(BF16)
    before = dot(named, earlier)
    targets_t = [
        ids_t[k : k + 1, :] * cap
        + jnp.sum(jnp.where(firsts[k], before, 0.0), axis=0, keepdims=True).astype(jnp.int32)
        for k in range(2)
    ]
    group = min(8, n_ep)

    @pl.loop(0, n_ep // group)
    def _(q):
        slots = lax.broadcasted_iota(jnp.int32, (group * cap, rows), 0) + q * group * cap
        place = jnp.where((slots == targets_t[0]) | (slots == targets_t[1]), 1.0, 0.0).astype(BF16)
        out_buf[pl.ds(q * group, group)] = (
            dot(place, xin[...]).astype(BF16).reshape(group, cap, width)
        )

    last = n_z - 1
    in_buf[2 * last + core] = out_buf[ep]

    pl.semaphore_wait(barrier, n_ep - 1 + n_tp - 1)

    for copy in shard_copies:
        copy.start()

    def token_copy(o, k):
        to = 2 * ((z + far_first(o, n_z)) % n_z) + k
        return pltpu.make_async_remote_copy(
            src_ref=out_buf.at[to],
            dst_ref=in_buf.at[2 * o + core],
            send_sem=tok_send.at[2 * o + k],
            recv_sem=tok_recv.at[2 * o + core],
            device_id={"ep": to},
            device_id_type=MESH,
        )

    def token_arrival(o, k):
        return pltpu.make_async_remote_copy(
            src_ref=in_buf.at[2 * o + k],
            dst_ref=in_buf.at[2 * o + k],
            send_sem=tok_send.at[2 * o + k],
            recv_sem=tok_recv.at[2 * o + k],
            device_id={"ep": 2 * z + 1 - core},
            device_id_type=MESH,
        )

    sibling = pltpu.make_async_remote_copy(
        src_ref=out_buf.at[2 * z + 1 - core],
        dst_ref=in_buf.at[2 * last + core],
        send_sem=tok_send.at[2 * last + 1 - core],
        recv_sem=tok_recv.at[2 * last + core],
        device_id={"ep": 2 * z + 1 - core},
        device_id_type=MESH,
    )
    sibling.start()

    @pl.loop(0, last)
    def _(o):
        for k in range(2):
            token_copy(o, k).start()

    loads[4].wait()
    loads[6].wait()
    normed[tp] = rms_rows(mrows[...], mgain[...])

    edge = pl.ds(rows - WINDOW_MAX, WINDOW_MAX)

    def tail_copy(r):
        return pltpu.make_async_remote_copy(
            src_ref=normed.at[n_tp - 1, edge],
            dst_ref=tail,
            send_sem=tail_send.at[r],
            recv_sem=tail_recv,
            device_id={"tp": (tp + r) % n_tp},
            device_id_type=MESH,
        )

    loads[7].wait()

    @pl.when(tp == n_tp - 1)
    def _():
        for r in (2, 1, 3):
            tail_copy(r).start()
        tail[...] = normed[n_tp - 1, edge]

    @pl.when(tp != n_tp - 1)
    def _():
        tail_copy(0).wait_recv()

    edge_out[...] = dot(tail[...], inw_v[...]).astype(BF16)
    halo = pltpu.make_async_remote_copy(
        src_ref=edge_out,
        dst_ref=edge_in,
        send_sem=halo_send,
        recv_sem=halo_recv,
        device_id={"ep": (ep + 1) % n_ep},
        device_id_type=MESH,
    )
    halo.start()

    def spread(r):
        return pltpu.make_async_remote_copy(
            src_ref=normed.at[tp],
            dst_ref=normed.at[tp],
            send_sem=ag_send.at[r],
            recv_sem=ag_recv.at[r],
            device_id={"tp": (tp + r) % n_tp},
            device_id_type=MESH,
        )

    groups = 4
    chips = n_z // groups
    per = 2 * chips
    half_rows = per * cap
    step = min(512, width)
    across = n_tp - 1 - tp

    def swap(o):
        return pltpu.make_async_remote_copy(
            src_ref=in_buf.at[pl.ds(2 * o, 2)],
            dst_ref=peer_buf.at[pl.ds(2 * o, 2)],
            send_sem=swap_send.at[o],
            recv_sem=swap_recv.at[o],
            device_id={"tp": across},
            device_id_type=MESH,
        )

    def pass_on(first, end):
        @pl.loop(first, min(end, last))
        def _(o):
            for k in range(2):
                token_arrival(o, k).wait_recv()
            swap(o).start()

        if end == n_z:
            token_arrival(last, 1 - core).wait_recv()
            swap(last).start()

    def partial_copy(g):
        return pltpu.make_async_remote_copy(
            src_ref=part_out.at[g],
            dst_ref=part_back.at[g],
            send_sem=back_send.at[g],
            recv_sem=back_recv.at[g],
            device_id={"tp": across},
            device_id_type=MESH,
        )

    def serve(g):
        @pl.loop(g * chips, (g + 1) * chips)
        def _(o):
            swap(o).wait_recv()

        mine = pl.ds(g * per, per)
        x = jnp.concatenate(
            [
                peer_buf[mine].reshape(half_rows, width),
                in_buf[mine].reshape(half_rows, width),
            ],
            axis=0,
        )
        hidden = []
        for s in range(2):
            gate_in = dot(x, wg[s])
            hidden.append((gate_in / (1.0 + jnp.exp(-gate_in)) * dot(x, wu[s])).astype(BF16))
        for c in range(0, width, step):
            total = dot(hidden[0], wd[0, :, c : c + step]).astype(BF16).astype(F32)
            total = total + dot(hidden[1], wd[1, :, c : c + step]).astype(BF16).astype(F32)
            part_out[g, :, c : c + step] = total[:half_rows].astype(BF16)
            acc[g, :, c : c + step] = total[half_rows:]
        partial_copy(g).start()

    def result_copy(o, k):
        to = 2 * ((z + n_z - far_first(o, n_z)) % n_z) + k
        return pltpu.make_async_remote_copy(
            src_ref=res_buf.at[2 * o + k],
            dst_ref=ret_buf.at[ep],
            send_sem=ret_send.at[2 * o + k],
            recv_sem=ret_recv.at[2 * o + core],
            device_id={"ep": to},
            device_id_type=MESH,
        )

    def result_arrival(o, k):
        sender = 2 * ((z + far_first(o, n_z)) % n_z) + k
        return pltpu.make_async_remote_copy(
            src_ref=res_buf.at[2 * o + k],
            dst_ref=ret_buf.at[sender],
            send_sem=ret_send.at[2 * o + k],
            recv_sem=ret_recv.at[2 * o + k],
            device_id={"ep": 2 * z + 1 - core},
            device_id_type=MESH,
        )

    sibling_back = pltpu.make_async_remote_copy(
        src_ref=res_buf.at[2 * last + 1 - core],
        dst_ref=ret_buf.at[ep],
        send_sem=ret_send.at[2 * last + 1 - core],
        recv_sem=ret_recv.at[2 * last + core],
        device_id={"ep": 2 * z + 1 - core},
        device_id_type=MESH,
    )

    def answer(g):
        partial_copy(g).wait_recv()
        res_buf[pl.ds(g * per, per)] = (
            (acc[g] + part_back[g].astype(F32)).astype(BF16).reshape(per, cap, width)
        )

        @pl.loop(g * chips, min((g + 1) * chips, last))
        def _(o):
            for k in range(2):
                result_copy(o, k).start()

        if g == groups - 1:
            sibling_back.start()
            ret_buf[ep] = res_buf[2 * last + core]

    pass_on(0, 3 * chips)
    for i in range(8, 11):
        loads[i].wait()
    for copy in shard_copies:
        copy.wait_recv()
    for g in range(groups - 1):
        serve(g)
    middle = 3 * chips + chips // 2
    pass_on(3 * chips, middle)
    answer(0)
    pass_on(middle, n_z)
    serve(groups - 1)
    for r in (2, 1, 3):
        spread(r).start()
    for g in range(1, groups):
        answer(g)

    for i in (3, 5, 11, 12):
        loads[i].wait()
    ext[0] = jnp.zeros((rows, ext.shape[2]), BF16)
    ext[tp + 1] = dot(normed[tp], inw_v[...]).astype(BF16)
    for r in (1, 3, 2):
        spread(r).wait_recv()
        src = (tp + n_tp - r) % n_tp
        ext[src + 1] = dot(normed[src], inw_v[...]).astype(BF16)
    window = jnp.left_shift(jnp.int32(2), tp)
    lag = lax.broadcasted_iota(jnp.int32, (rows, rows), 0) - lax.broadcasted_iota(
        jnp.int32, (rows, rows), 1
    )
    band = jnp.where((lag >= 0) & (lag < window), 1.0, 0.0).astype(BF16)
    band_before = jnp.where(lag + rows < window, 1.0, 0.0).astype(BF16)
    place_in = lax.broadcasted_iota(jnp.int32, (rows, 1), 0) + 1
    halo.wait_recv()
    ext[0, edge, :] = jnp.where(ep == 0, 0.0, edge_in[...].astype(F32)).astype(BF16)

    def sums(r):
        to = (tp + r) % n_tp
        return pltpu.make_async_remote_copy(
            src_ref=part_buf.at[to],
            dst_ref=part_in.at[r - 1],
            send_sem=rs_send.at[r],
            recv_sem=rs_recv.at[r],
            device_id={"tp": to},
            device_id_type=MESH,
        )

    for r in (2, 1, 3, 0):
        m = (tp + r) % n_tp
        here = ext[m + 1]
        total = dot(band, here) + dot(band_before, ext[m])
        counts = jnp.minimum(place_in + (ep * n_tp + m) * rows, window).astype(F32)
        pooled = (total / counts - here.astype(F32)).astype(BF16)
        grouped = (dot(pooled, gw_v[...]) * scale[...].astype(F32)[None]).astype(BF16)
        for c in range(0, width, step):
            part_buf[m, :, c : c + step] = dot(grouped, ow_v[:, c : c + step]).astype(BF16)
        if r:
            sums(r).start()

    for r in (1, 3, 2):
        sums(r).wait_recv()
    total = part_buf[tp].astype(F32)
    for r in range(n_tp - 1):
        total = total + part_in[r].astype(F32)
    mixed_out[...] = total.astype(BF16)

    ids = jnp.transpose(ids_t[...])
    shares = jnp.transpose(shares_t[...])
    lanes = lax.broadcasted_iota(jnp.int32, (rows, n_ep), 1)
    mine = [ids[:, k : k + 1] == lanes for k in range(2)]
    named_rows = jnp.where(mine[0] | mine[1], 1.0, 0.0).astype(BF16)
    later = jnp.where(lag > 0, 1.0, 0.0).astype(BF16)
    before_rows = dot(later, named_rows)
    slots = lax.broadcasted_iota(jnp.int32, (rows, n_slots), 1)
    picks = []
    for k in range(2):
        target = ids[:, k : k + 1] * cap + jnp.sum(
            jnp.where(mine[k], before_rows, 0.0), axis=1, keepdims=True
        ).astype(jnp.int32)
        picks.append(jnp.where(slots == target, 1.0, 0.0).astype(BF16))
    weight = shares / jnp.sum(shares, axis=1, keepdims=True)

    @pl.loop(0, last)
    def _(o):
        for k in range(2):
            result_arrival(o, k).wait_recv()

    pltpu.make_async_remote_copy(
        src_ref=res_buf.at[2 * last + 1 - core],
        dst_ref=ret_buf.at[2 * z + 1 - core],
        send_sem=ret_send.at[2 * last + 1 - core],
        recv_sem=ret_recv.at[2 * last + 1 - core],
        device_id={"ep": 2 * z + 1 - core},
        device_id_type=MESH,
    ).wait_recv()

    for c in range(0, width, step):
        back = ret_buf[:, :, c : c + step].reshape(n_slots, step)
        mix = dot(picks[0], back) * weight[:, 0:1] + dot(picks[1], back) * weight[:, 1:2]
        expert_out[:, c : c + step] = mix.astype(BF16)

    for copy in (*shard_copies, sibling, sibling_back):
        copy.wait_send()

    @pl.loop(0, last)
    def _(o):
        for k in range(2):
            token_copy(o, k).wait_send()
            result_copy(o, k).wait_send()

    @pl.loop(0, n_z)
    def _(o):
        swap(o).wait_send()

    for g in range(groups):
        partial_copy(g).wait_send()

    for r in range(1, n_tp):
        spread(r).wait_send()
        sums(r).wait_send()
    halo.wait_send()

    @pl.when(tp == n_tp - 1)
    def _():
        for r in range(1, n_tp):
            tail_copy(r).wait_send()


def solution(mesh):
    n_ep, n_tp = mesh.shape["ep"], mesh.shape["tp"]

    def local(
        mixer_tokens, mixer_gain, in_weight, group_weight, channel_scale, out_weight,
        expert_tokens, expert_gain, route_ids, route_weights, gate_weight, up_weight, down_weight,
    ):
        rows, width = expert_tokens.shape
        cap = 4 * rows // n_ep
        gw = in_weight.shape[1]
        ff = gate_weight.shape[2]
        vmem = pl.BlockSpec(memory_space=pltpu.VMEM)
        hbm = pl.BlockSpec(memory_space=pl.ANY)
        slots = n_ep * cap
        V = pltpu.VMEM
        dma = pltpu.SemaphoreType.DMA
        out = jax.ShapeDtypeStruct((rows, width), BF16)
        return pl.pallas_call(
            functools.partial(kernel, n_ep, n_tp, cap),
            out_shape=(out, out),
            in_specs=[hbm] * 13,
            out_specs=(vmem, vmem),
            scratch_shapes=[
                V((rows, width), BF16),
                V((width,), BF16),
                V((width,), BF16),
                V((gw,), BF16),
                V((2, rows), jnp.int32),
                V((2, rows), F32),
                V((rows, width), BF16),
                V((n_ep, cap, width), BF16),
                V((n_ep, cap, width), BF16),
                V((n_ep, cap, width), BF16),
                V((n_ep, cap, width), BF16),
                V((n_ep, cap, width), BF16),
                V((4, slots // 4, width), F32),
                V((4, slots // 4, width), BF16),
                V((4, slots // 4, width), BF16),
                V((2, width, ff), BF16),
                V((2, width, ff), BF16),
                V((2, ff, width), BF16),
                V((rows, width), BF16),
                V((n_tp, rows, width), BF16),
                V((WINDOW_MAX, width), BF16),
                V((WINDOW_MAX, gw), BF16),
                V((WINDOW_MAX, gw), BF16),
                V((width, gw), BF16),
                V((gw, gw), BF16),
                V((gw, width), BF16),
                V((n_tp + 1, rows, gw), BF16),
                V((n_tp, rows, width), BF16),
                V((n_tp - 1, rows, width), BF16),
                dma((13,)),
                dma((n_ep,)),
                dma((n_ep,)),
                dma((n_ep // 2,)),
                dma((n_ep // 2,)),
                dma((4,)),
                dma((4,)),
                dma((n_ep,)),
                dma((n_ep,)),
                dma((3,)),
                dma((3,)),
                dma((n_tp,)),
                dma((n_tp,)),
                dma((n_tp,)),
                dma,
                dma,
                dma,
                dma((n_tp,)),
                dma((n_tp,)),
            ],
            compiler_params=pltpu.CompilerParams(
                collective_id=0, has_side_effects=True, vmem_limit_bytes=52 * 1024 * 1024
            ),
        )(
            *(
                pltpu.with_memory_space_constraint(a, pltpu.HBM)
                for a in (
                    mixer_tokens, mixer_gain, in_weight, group_weight, channel_scale, out_weight,
                    expert_tokens, expert_gain, route_ids.T, route_weights.T,
                    gate_weight, up_weight, down_weight,
                )
            )
        )

    block = P(("grp", "ep", "tp"), None)
    placed = (
        block, P(), P(None, "tp"), P("tp", None, None), P("tp"), P("tp", None),
        block, P(), block, block, P("ep", None, "tp"), P("ep", None, "tp"), P("ep", "tp", None),
    )
    return jax.shard_map(
        local, mesh=mesh, in_specs=placed, out_specs=(block, block), check_vma=False
    )
```

```python
import functools

import jax
import jax.numpy as jnp
from jax import lax
from jax.experimental import pallas as pl
from jax.experimental.pallas import tpu as pltpu
from jax.sharding import PartitionSpec as P

MESH = pl.DeviceIdType.MESH
F32 = jnp.float32
BF16 = jnp.bfloat16
WINDOW_MAX = 16


def dot(a, b):
    return jnp.dot(a, b, preferred_element_type=F32)


def rms_rows(rows, gain):
    values = rows.astype(F32)
    scaled = values * lax.rsqrt(jnp.mean(values * values, axis=-1, keepdims=True) + 1e-06)
    return (scaled * gain.astype(F32)[None]).astype(BF16)


def offset(j, n):
    if not isinstance(j, int):
        pair, i = j // 4, j % 4
        hops = (1 - i // 2) * (n // 2 - 1 - pair) + (i // 2) * (1 + pair)
        return (n + (1 - 2 * (i % 2)) * hops) % n
    return (n // 2, n // 4, 3 * n // 4, 0)[j - n + 4]


def kernel(
    n_ep, n_tp, cap,
    mtok, mgain_h, inw, gw, scale_h, ow, etok_h, egain_h, ids_h, shares_h, gate, up, down,
    mixed_out, expert_out,
    etok, egain, mgain, scale, ids_t, shares_t,
    xin, out_buf, in_buf, peer_buf, res_buf, ret_buf, acc, part_out, part_back, wg, wu, wd,
    mrows, normed, tail, edge_out, edge_in, inw_v, gw_v, ow_v, ext, part_buf, part_in,
    load_sem, tok_send, tok_recv, swap_send, swap_recv, back_send, back_recv,
    ret_send, ret_recv, w_send, w_recv,
    ag_send, ag_recv, tail_send, tail_recv, halo_send, halo_recv, rs_send, rs_recv,
):
    ep = lax.axis_index("ep")
    tp = lax.axis_index("tp")
    rows, width = mtok.shape
    n_slots = n_ep * cap
    beside, across = tp + 1 - 2 * (tp % 2), n_tp - 1 - tp
    opposite = n_tp - 1 - beside
    n_z = n_ep // 2
    z, core = ep // 2, ep % 2

    barrier = pltpu.get_barrier_semaphore()

    @pl.loop(1, n_ep)
    def _(r):
        pl.semaphore_signal(
            barrier, inc=1, device_id={"ep": (ep + r) % n_ep}, device_id_type=MESH
        )

    for r in range(1, n_tp):
        pl.semaphore_signal(
            barrier, inc=1, device_id={"tp": (tp + r) % n_tp}, device_id_type=MESH
        )

    loads = [
        pltpu.make_async_copy(src, dst, load_sem.at[i])
        for i, (src, dst) in enumerate(
            [
                (etok_h, etok),
                (egain_h, egain),
                (ids_h, ids_t),
                (shares_h, shares_t),
                (mgain_h, mgain),
                (scale_h, scale),
                (mtok, mrows),
                (inw, inw_v),
                (gate.at[0], wg.at[0]),
                (up.at[0], wu.at[0]),
                (down.at[0], wd.at[0]),
                (gw.at[0], gw_v),
                (ow, ow_v),
            ]
        )
    ]
    for load in loads:
        load.start()
    for i in range(3):
        loads[i].wait()

    def weights(i, src, dst):
        return pltpu.make_async_remote_copy(
            src_ref=src,
            dst_ref=dst,
            send_sem=w_send.at[i],
            recv_sem=w_recv.at[i],
            device_id={"tp": beside},
            device_id_type=MESH,
        )

    shard_copies = [
        weights(0, gate.at[0], wg.at[1]),
        weights(1, up.at[0], wu.at[1]),
        weights(2, down.at[0], wd.at[1]),
    ]

    xin[...] = rms_rows(etok[...], egain[...])
    experts = lax.broadcasted_iota(jnp.int32, (n_ep, rows), 0)
    firsts = [ids_t[k : k + 1, :] == experts for k in range(2)]
    named = jnp.where(firsts[0] | firsts[1], 1.0, 0.0).astype(BF16)
    earlier = jnp.where(
        lax.broadcasted_iota(jnp.int32, (rows, rows), 0)
        < lax.broadcasted_iota(jnp.int32, (rows, rows), 1),
        1.0,
        0.0,
    ).astype(BF16)
    before = dot(named, earlier)
    targets_t = [
        ids_t[k : k + 1, :] * cap
        + jnp.sum(jnp.where(firsts[k], before, 0.0), axis=0, keepdims=True).astype(jnp.int32)
        for k in range(2)
    ]
    group = min(8, n_ep)

    @pl.loop(0, n_ep // group)
    def _(q):
        slots = lax.broadcasted_iota(jnp.int32, (group * cap, rows), 0) + q * group * cap
        place = jnp.where((slots == targets_t[0]) | (slots == targets_t[1]), 1.0, 0.0).astype(BF16)
        out_buf[pl.ds(q * group, group)] = (
            dot(place, xin[...]).astype(BF16).reshape(group, cap, width)
        )

    last = n_z - 1
    in_buf[2 * last + core] = out_buf[ep]

    def each(first, end, work):
        if first < n_z - 4:
            pl.loop(first, min(end, n_z - 4))(work)
        for o in range(max(first, n_z - 4), min(end, last)):
            work(o)

    pl.semaphore_wait(barrier, n_ep - 1 + n_tp - 1)

    def token_copy(o, k):
        to = 2 * ((z + offset(o, n_z)) % n_z) + k
        return pltpu.make_async_remote_copy(
            src_ref=out_buf.at[to],
            dst_ref=in_buf.at[2 * o + core],
            send_sem=tok_send.at[2 * o + k],
            recv_sem=tok_recv.at[2 * o + core],
            device_id={"ep": to},
            device_id_type=MESH,
        )

    def token_arrival(o, k):
        return pltpu.make_async_remote_copy(
            src_ref=in_buf.at[2 * o + k],
            dst_ref=in_buf.at[2 * o + k],
            send_sem=tok_send.at[2 * o + k],
            recv_sem=tok_recv.at[2 * o + k],
            device_id={"ep": 2 * z + 1 - core},
            device_id_type=MESH,
        )

    sibling = pltpu.make_async_remote_copy(
        src_ref=out_buf.at[2 * z + 1 - core],
        dst_ref=in_buf.at[2 * last + core],
        send_sem=tok_send.at[2 * last + 1 - core],
        recv_sem=tok_recv.at[2 * last + core],
        device_id={"ep": 2 * z + 1 - core},
        device_id_type=MESH,
    )
    sibling.start()

    def send_tokens(o):
        for k in range(2):
            token_copy(o, k).start()

    each(0, last, send_tokens)
    shard_copies[0].start()

    loads[4].wait()
    loads[6].wait()
    normed[tp] = rms_rows(mrows[...], mgain[...])

    edge = pl.ds(rows - WINDOW_MAX, WINDOW_MAX)

    def tail_copy(r):
        return pltpu.make_async_remote_copy(
            src_ref=normed.at[n_tp - 1, edge],
            dst_ref=tail,
            send_sem=tail_send.at[r],
            recv_sem=tail_recv,
            device_id={"tp": (tp + r) % n_tp},
            device_id_type=MESH,
        )

    loads[7].wait()

    @pl.when(tp == n_tp - 1)
    def _():
        for r in (2, 1, 3):
            tail_copy(r).start()
        tail[...] = normed[n_tp - 1, edge]

    for copy in shard_copies[1:]:
        copy.start()

    def spread(i, src, to):
        return pltpu.make_async_remote_copy(
            src_ref=normed.at[src],
            dst_ref=normed.at[src],
            send_sem=ag_send.at[i],
            recv_sem=ag_recv.at[i],
            device_id={"tp": to},
            device_id_type=MESH,
        )

    def spread_arrival(i, src):
        return spread(i, src, across)

    spreads = [spread(0, tp, across), spread(1, tp, beside), spread(2, across, beside)]
    spreads[0].start()
    spreads[1].start()

    groups = 4
    chips = n_z // groups
    per = 2 * chips
    half_rows = per * cap
    step = min(512, width)

    def swap(o):
        return pltpu.make_async_remote_copy(
            src_ref=in_buf.at[pl.ds(2 * o, 2)],
            dst_ref=peer_buf.at[pl.ds(2 * o, 2)],
            send_sem=swap_send.at[o],
            recv_sem=swap_recv.at[o],
            device_id={"tp": across},
            device_id_type=MESH,
        )

    def pass_on(o):
        for k in range(2):
            token_arrival(o, k).wait_recv()
        swap(o).start()

    def partial_copy(g):
        return pltpu.make_async_remote_copy(
            src_ref=part_out.at[g],
            dst_ref=part_back.at[g],
            send_sem=back_send.at[g],
            recv_sem=back_recv.at[g],
            device_id={"tp": across},
            device_id_type=MESH,
        )

    def serve(g):
        @pl.loop(g * chips, (g + 1) * chips)
        def _(o):
            swap(o).wait_recv()

        mine = pl.ds(g * per, per)
        x = jnp.concatenate(
            [
                peer_buf[mine].reshape(half_rows, width),
                in_buf[mine].reshape(half_rows, width),
            ],
            axis=0,
        )
        hidden = []
        for s in range(2):
            gate_in = dot(x, wg[s])
            hidden.append((gate_in / (1.0 + jnp.exp(-gate_in)) * dot(x, wu[s])).astype(BF16))
        for c in range(0, width, step):
            total = dot(hidden[0], wd[0, :, c : c + step]).astype(BF16).astype(F32)
            total = total + dot(hidden[1], wd[1, :, c : c + step]).astype(BF16).astype(F32)
            part_out[g, :, c : c + step] = total[:half_rows].astype(BF16)
            acc[g, :, c : c + step] = total[half_rows:]
        partial_copy(g).start()

    def result_copy(o, k):
        to = 2 * ((z + n_z - offset(o, n_z)) % n_z) + k
        return pltpu.make_async_remote_copy(
            src_ref=res_buf.at[2 * o + k],
            dst_ref=ret_buf.at[ep],
            send_sem=ret_send.at[2 * o + k],
            recv_sem=ret_recv.at[2 * o + core],
            device_id={"ep": to},
            device_id_type=MESH,
        )

    def result_arrival(o, k):
        sender = 2 * ((z + offset(o, n_z)) % n_z) + k
        return pltpu.make_async_remote_copy(
            src_ref=res_buf.at[2 * o + k],
            dst_ref=ret_buf.at[sender],
            send_sem=ret_send.at[2 * o + k],
            recv_sem=ret_recv.at[2 * o + k],
            device_id={"ep": 2 * z + 1 - core},
            device_id_type=MESH,
        )

    sibling_back = pltpu.make_async_remote_copy(
        src_ref=res_buf.at[2 * last + 1 - core],
        dst_ref=ret_buf.at[ep],
        send_sem=ret_send.at[2 * last + 1 - core],
        recv_sem=ret_recv.at[2 * last + core],
        device_id={"ep": 2 * z + 1 - core},
        device_id_type=MESH,
    )

    def answer(g):
        partial_copy(g).wait_recv()
        res_buf[pl.ds(g * per, per)] = (
            (acc[g] + part_back[g].astype(F32)).astype(BF16).reshape(per, cap, width)
        )

        def send_results(o):
            for k in range(2):
                result_copy(o, k).start()

        each(g * chips, (g + 1) * chips, send_results)
        if g == groups - 1:
            sibling_back.start()
            ret_buf[ep] = res_buf[2 * last + core]

    token_arrival(last, 1 - core).wait_recv()
    swap(last).start()
    each(0, 2 * chips, pass_on)

    @pl.when(tp != n_tp - 1)
    def _():
        tail_copy(0).wait_recv()

    edge_out[...] = dot(tail[...], inw_v[...]).astype(BF16)
    halo = pltpu.make_async_remote_copy(
        src_ref=edge_out,
        dst_ref=edge_in,
        send_sem=halo_send,
        recv_sem=halo_recv,
        device_id={"ep": (ep + 1) % n_ep},
        device_id_type=MESH,
    )
    halo.start()
    spread_arrival(0, across).wait_recv()
    spreads[2].start()

    each(2 * chips, 3 * chips, pass_on)
    for i in range(8, 11):
        loads[i].wait()
    for copy in shard_copies:
        copy.wait_recv()
    serve(0)
    serve(1)
    answer(0)
    each(3 * chips, last, pass_on)
    serve(2)
    answer(1)
    serve(3)
    answer(2)

    for i in (3, 5, 11, 12):
        loads[i].wait()
    ext[0] = jnp.zeros((rows, ext.shape[2]), BF16)
    for i, src in enumerate((across, beside, opposite)):
        if i:
            spread_arrival(i, src).wait_recv()
        ext[src + 1] = dot(normed[src], inw_v[...]).astype(BF16)
    ext[tp + 1] = dot(normed[tp], inw_v[...]).astype(BF16)
    window = jnp.left_shift(jnp.int32(2), tp)
    lag = lax.broadcasted_iota(jnp.int32, (rows, rows), 0) - lax.broadcasted_iota(
        jnp.int32, (rows, rows), 1
    )
    band = jnp.where((lag >= 0) & (lag < window), 1.0, 0.0).astype(BF16)
    band_before = jnp.where(lag + rows < window, 1.0, 0.0).astype(BF16)
    place_in = lax.broadcasted_iota(jnp.int32, (rows, 1), 0) + 1
    halo.wait_recv()
    ext[0, edge, :] = jnp.where(ep == 0, 0.0, edge_in[...].astype(F32)).astype(BF16)

    def sums(i, src, to):
        return pltpu.make_async_remote_copy(
            src_ref=part_buf.at[src],
            dst_ref=part_in.at[i],
            send_sem=rs_send.at[i],
            recv_sem=rs_recv.at[i],
            device_id={"tp": to},
            device_id_type=MESH,
        )

    parts = [sums(0, beside, beside), sums(1, opposite, beside), sums(2, across, across)]
    for i, m in ((1, opposite), (0, beside), (2, across), (3, tp)):
        here = ext[m + 1]
        total = dot(band, here) + dot(band_before, ext[m])
        counts = jnp.minimum(place_in + (ep * n_tp + m) * rows, window).astype(F32)
        pooled = (total / counts - here.astype(F32)).astype(BF16)
        grouped = (dot(pooled, gw_v[...]) * scale[...].astype(F32)[None]).astype(BF16)
        for c in range(0, width, step):
            part_buf[m, :, c : c + step] = dot(grouped, ow_v[:, c : c + step]).astype(BF16)
        if i < 2:
            parts[i].start()

    answer(3)

    parts[1].wait_recv()
    part_buf[across] = (part_buf[across].astype(F32) + part_in[1].astype(F32)).astype(BF16)
    parts[2].start()
    parts[0].wait_recv()
    parts[2].wait_recv()
    mixed_out[...] = (
        part_buf[tp].astype(F32) + part_in[0].astype(F32) + part_in[2].astype(F32)
    ).astype(BF16)

    ids = jnp.transpose(ids_t[...])
    shares = jnp.transpose(shares_t[...])
    lanes = lax.broadcasted_iota(jnp.int32, (rows, n_ep), 1)
    mine = [ids[:, k : k + 1] == lanes for k in range(2)]
    named_rows = jnp.where(mine[0] | mine[1], 1.0, 0.0).astype(BF16)
    later = jnp.where(lag > 0, 1.0, 0.0).astype(BF16)
    before_rows = dot(later, named_rows)
    slots = lax.broadcasted_iota(jnp.int32, (rows, n_slots), 1)
    picks = []
    for k in range(2):
        target = ids[:, k : k + 1] * cap + jnp.sum(
            jnp.where(mine[k], before_rows, 0.0), axis=1, keepdims=True
        ).astype(jnp.int32)
        picks.append(jnp.where(slots == target, 1.0, 0.0).astype(BF16))
    weight = shares / jnp.sum(shares, axis=1, keepdims=True)

    def await_results(o):
        for k in range(2):
            result_arrival(o, k).wait_recv()

    each(0, last, await_results)
    pltpu.make_async_remote_copy(
        src_ref=res_buf.at[2 * last + 1 - core],
        dst_ref=ret_buf.at[2 * z + 1 - core],
        send_sem=ret_send.at[2 * last + 1 - core],
        recv_sem=ret_recv.at[2 * last + 1 - core],
        device_id={"ep": 2 * z + 1 - core},
        device_id_type=MESH,
    ).wait_recv()

    for c in range(0, width, step):
        back = ret_buf[:, :, c : c + step].reshape(n_slots, step)
        mix = dot(picks[0], back) * weight[:, 0:1] + dot(picks[1], back) * weight[:, 1:2]
        expert_out[:, c : c + step] = mix.astype(BF16)

    for copy in (*shard_copies, sibling, sibling_back):
        copy.wait_send()

    def await_sent(o):
        for k in range(2):
            token_copy(o, k).wait_send()
            result_copy(o, k).wait_send()

    each(0, last, await_sent)

    @pl.loop(0, n_z)
    def _(o):
        swap(o).wait_send()

    for g in range(groups):
        partial_copy(g).wait_send()

    for copy in (*spreads, *parts):
        copy.wait_send()
    halo.wait_send()

    @pl.when(tp == n_tp - 1)
    def _():
        for r in range(1, n_tp):
            tail_copy(r).wait_send()


def solution(mesh):
    n_ep, n_tp = mesh.shape["ep"], mesh.shape["tp"]

    def local(
        mixer_tokens, mixer_gain, in_weight, group_weight, channel_scale, out_weight,
        expert_tokens, expert_gain, route_ids, route_weights, gate_weight, up_weight, down_weight,
    ):
        rows, width = expert_tokens.shape
        cap = 4 * rows // n_ep
        gw = in_weight.shape[1]
        ff = gate_weight.shape[2]
        vmem = pl.BlockSpec(memory_space=pltpu.VMEM)
        hbm = pl.BlockSpec(memory_space=pl.ANY)
        slots = n_ep * cap
        V = pltpu.VMEM
        dma = pltpu.SemaphoreType.DMA
        out = jax.ShapeDtypeStruct((rows, width), BF16)
        return pl.pallas_call(
            functools.partial(kernel, n_ep, n_tp, cap),
            out_shape=(out, out),
            in_specs=[hbm] * 13,
            out_specs=(vmem, vmem),
            scratch_shapes=[
                V((rows, width), BF16),
                V((width,), BF16),
                V((width,), BF16),
                V((gw,), BF16),
                V((2, rows), jnp.int32),
                V((2, rows), F32),
                V((rows, width), BF16),
                V((n_ep, cap, width), BF16),
                V((n_ep, cap, width), BF16),
                V((n_ep, cap, width), BF16),
                V((n_ep, cap, width), BF16),
                V((n_ep, cap, width), BF16),
                V((4, slots // 4, width), F32),
                V((4, slots // 4, width), BF16),
                V((4, slots // 4, width), BF16),
                V((2, width, ff), BF16),
                V((2, width, ff), BF16),
                V((2, ff, width), BF16),
                V((rows, width), BF16),
                V((n_tp, rows, width), BF16),
                V((WINDOW_MAX, width), BF16),
                V((WINDOW_MAX, gw), BF16),
                V((WINDOW_MAX, gw), BF16),
                V((width, gw), BF16),
                V((gw, gw), BF16),
                V((gw, width), BF16),
                V((n_tp + 1, rows, gw), BF16),
                V((n_tp, rows, width), BF16),
                V((n_tp - 1, rows, width), BF16),
                dma((13,)),
                dma((n_ep,)),
                dma((n_ep,)),
                dma((n_ep // 2,)),
                dma((n_ep // 2,)),
                dma((4,)),
                dma((4,)),
                dma((n_ep,)),
                dma((n_ep,)),
                dma((3,)),
                dma((3,)),
                dma((n_tp,)),
                dma((n_tp,)),
                dma((n_tp,)),
                dma,
                dma,
                dma,
                dma((n_tp,)),
                dma((n_tp,)),
            ],
            compiler_params=pltpu.CompilerParams(
                collective_id=0, has_side_effects=True, vmem_limit_bytes=52 * 1024 * 1024
            ),
        )(
            *(
                pltpu.with_memory_space_constraint(a, pltpu.HBM)
                for a in (
                    mixer_tokens, mixer_gain, in_weight, group_weight, channel_scale, out_weight,
                    expert_tokens, expert_gain, route_ids.T, route_weights.T,
                    gate_weight, up_weight, down_weight,
                )
            )
        )

    block = P(("grp", "ep", "tp"), None)
    placed = (
        block, P(), P(None, "tp"), P("tp", None, None), P("tp"), P("tp", None),
        block, P(), block, block, P("ep", None, "tp"), P("ep", None, "tp"), P("ep", "tp", None),
    )
    return jax.shard_map(
        local, mesh=mesh, in_specs=placed, out_specs=(block, block), check_vma=False
    )
```

```python
import functools

import jax
import jax.numpy as jnp
from jax import lax
from jax.experimental import pallas as pl
from jax.experimental.pallas import tpu as pltpu
from jax.sharding import PartitionSpec as P

MESH = pl.DeviceIdType.MESH
F32 = jnp.float32
BF16 = jnp.bfloat16
WINDOW_MAX = 16


def dot(a, b):
    return jnp.dot(a, b, preferred_element_type=F32)


def rms_rows(rows, gain):
    values = rows.astype(F32)
    scaled = values * lax.rsqrt(jnp.mean(values * values, axis=-1, keepdims=True) + 1e-06)
    return (scaled * gain.astype(F32)[None]).astype(BF16)


def offset(j, n):
    if not isinstance(j, int) or j < n - 4:
        pair, i = j // 4, j % 4
        hops = (1 - i // 2) * (n // 2 - 1 - pair) + (i // 2) * (1 + pair)
        return (n + (1 - 2 * (i % 2)) * hops) % n
    return (n // 2, n // 4, 3 * n // 4, 0)[j - n + 4]


def kernel(
    n_ep, n_tp, cap,
    mtok, mgain_h, inw, gw, scale_h, ow, etok_h, egain_h, ids_h, shares_h, gate, up, down,
    mixed_out, expert_out,
    etok, egain, mgain, scale, ids_t, shares_t,
    xin, meta, own_buf, stream, meta_in, relay, in_buf, peer_buf, res_buf, ret_buf, hidden, acc, part_out, part_back, wg, wu, wd,
    mrows, normed, tail, edge_out, edge_in, inw_v, gw_v, ow_v, ext, part_buf, part_in,
    load_sem, stream_send, stream_recv, tok_send, tok_recv, swap_send, swap_recv, back_send, back_recv,
    ret_send, ret_recv, w_send, w_recv,
    ag_send, ag_recv, tail_send, tail_recv, halo_send, halo_recv, rs_send, rs_recv,
):
    ep = lax.axis_index("ep")
    tp = lax.axis_index("tp")
    rows, width = mtok.shape
    n_slots = n_ep * cap
    beside, across = tp + 1 - 2 * (tp % 2), n_tp - 1 - tp
    opposite = n_tp - 1 - beside
    n_z = n_ep // 2
    z, core = ep // 2, ep % 2

    barrier = pltpu.get_barrier_semaphore()

    @pl.loop(1, n_ep)
    def _(r):
        pl.semaphore_signal(
            barrier, inc=1, device_id={"ep": (ep + r) % n_ep}, device_id_type=MESH
        )

    for r in range(1, n_tp):
        pl.semaphore_signal(
            barrier, inc=1, device_id={"tp": (tp + r) % n_tp}, device_id_type=MESH
        )

    loads = [
        pltpu.make_async_copy(src, dst, load_sem.at[i])
        for i, (src, dst) in enumerate(
            [
                (etok_h, etok),
                (egain_h, egain),
                (ids_h, ids_t),
                (shares_h, shares_t),
                (mgain_h, mgain),
                (scale_h, scale),
                (mtok, mrows),
                (inw, inw_v),
                (gate.at[0], wg.at[0]),
                (up.at[0], wu.at[0]),
                (down.at[0], wd.at[0]),
                (gw.at[0], gw_v),
                (ow, ow_v),
            ]
        )
    ]
    for load in loads:
        load.start()
    for i in range(3):
        loads[i].wait()

    def weights(i, src, dst):
        return pltpu.make_async_remote_copy(
            src_ref=src,
            dst_ref=dst,
            send_sem=w_send.at[i],
            recv_sem=w_recv.at[i],
            device_id={"tp": beside},
            device_id_type=MESH,
        )

    shard_copies = [
        weights(0, gate.at[0], wg.at[1]),
        weights(1, up.at[0], wu.at[1]),
        weights(2, down.at[0], wd.at[1]),
    ]

    xin[...] = rms_rows(etok[...], egain[...])
    experts = lax.broadcasted_iota(jnp.int32, (n_ep, rows), 0)
    firsts = [ids_t[k : k + 1, :] == experts for k in range(2)]
    named = jnp.where(firsts[0] | firsts[1], 1.0, 0.0).astype(BF16)
    earlier = jnp.where(
        lax.broadcasted_iota(jnp.int32, (rows, rows), 0)
        < lax.broadcasted_iota(jnp.int32, (rows, rows), 1),
        1.0,
        0.0,
    ).astype(BF16)
    before = dot(named, earlier)
    targets_t = [
        ids_t[k : k + 1, :] * cap
        + jnp.sum(jnp.where(firsts[k], before, 0.0), axis=0, keepdims=True).astype(jnp.int32)
        for k in range(2)
    ]
    for k in range(2):
        meta[k : k + 1, :] = targets_t[k].astype(F32)

    def pick(tokens, targets, first, count):
        place = lax.broadcasted_iota(jnp.int32, (count * cap, rows), 0) + first * cap
        place = jnp.where(place >= n_slots, place - n_slots, place).astype(F32)
        chosen = jnp.where(
            (place == targets[0:1, :]) | (place == targets[1:2, :]), 1.0, 0.0
        ).astype(BF16)
        return lambda c: dot(chosen, tokens[:, c : c + step]).astype(BF16).reshape(count, cap, step)

    step = min(512, width)
    own = pick(xin, meta[...], 2 * z, 2)
    for c in range(0, width, step):
        own_buf[:, :, c : c + step] = own(c)
    last = n_z - 1
    in_buf[2 * last + core] = own_buf[core]
    order = [offset(o, n_z) for o in range(n_z)]
    ahead = [(z + 1) % n_z, (z + n_z - 1) % n_z]

    def each(first, end, work):
        if first < n_z - 4:
            pl.loop(first, min(end, n_z - 4))(work)
        for o in range(max(first, n_z - 4), min(end, last)):
            work(o)

    def along(side, i, src, dst):
        return pltpu.make_async_remote_copy(
            src_ref=src,
            dst_ref=dst,
            send_sem=stream_send.at[2 * side + i],
            recv_sem=stream_recv.at[2 * side + i],
            device_id={"ep": 2 * ahead[side] + core},
            device_id_type=MESH,
        )

    streams = [
        copy
        for side in range(2)
        for copy in (
            along(side, 0, meta, meta_in.at[side]),
            along(side, 1, xin, stream.at[side]),
        )
    ]

    pl.semaphore_wait(barrier, n_ep - 1 + n_tp - 1)

    for copy in streams:
        copy.start()

    def to_sibling(o, src):
        return pltpu.make_async_remote_copy(
            src_ref=src,
            dst_ref=in_buf.at[2 * o + core],
            send_sem=tok_send.at[2 * o + 1 - core],
            recv_sem=tok_recv.at[2 * o + core],
            device_id={"ep": 2 * z + 1 - core},
            device_id_type=MESH,
        )

    def relayed(o, k, side, block):
        to = 2 * ((z + order[o] + n_z + (-1, 1)[side]) % n_z) + k
        return pltpu.make_async_remote_copy(
            src_ref=relay.at[side, block],
            dst_ref=in_buf.at[2 * o + core],
            send_sem=tok_send.at[2 * o + k],
            recv_sem=tok_recv.at[2 * o + core],
            device_id={"ep": to},
            device_id_type=MESH,
        )

    def token_arrival(o, k):
        return pltpu.make_async_remote_copy(
            src_ref=in_buf.at[2 * o + k],
            dst_ref=in_buf.at[2 * o + k],
            send_sem=tok_send.at[2 * o + k],
            recv_sem=tok_recv.at[2 * o + k],
            device_id={"ep": 2 * z + 1 - core},
            device_id_type=MESH,
        )

    half = n_z // 2
    blocks = n_z - 1
    near = [order.index(1), order.index(n_z - 1)]
    here_at = [0, blocks - 2]
    relays = [[], []]
    for o in range(last):
        d = order[o]
        for k in range(2):
            if 2 <= d < half or (d == half and k == 0):
                relays[0].append(relayed(o, k, 0, 2 * (d - 1) + k))
            elif half < d <= n_z - 2 or d == half:
                relays[1].append(relayed(o, k, 1, 2 * (half - (n_z - d)) + k - 1))
    siblings = [to_sibling(last, own_buf.at[1 - core])] + [
        to_sibling(near[side], relay.at[side, here_at[side] + 1 - core]) for side in range(2)
    ]
    siblings[0].start()
    shard_copies[0].start()

    loads[4].wait()
    loads[6].wait()
    normed[tp] = rms_rows(mrows[...], mgain[...])

    edge = pl.ds(rows - WINDOW_MAX, WINDOW_MAX)

    def tail_copy(r):
        return pltpu.make_async_remote_copy(
            src_ref=normed.at[n_tp - 1, edge],
            dst_ref=tail,
            send_sem=tail_send.at[r],
            recv_sem=tail_recv,
            device_id={"tp": (tp + r) % n_tp},
            device_id_type=MESH,
        )

    loads[7].wait()

    @pl.when(tp == n_tp - 1)
    def _():
        for r in (2, 1, 3):
            tail_copy(r).start()
        tail[...] = normed[n_tp - 1, edge]

    for copy in shard_copies[1:]:
        copy.start()

    def spread(i, src, to):
        return pltpu.make_async_remote_copy(
            src_ref=normed.at[src],
            dst_ref=normed.at[src],
            send_sem=ag_send.at[i],
            recv_sem=ag_recv.at[i],
            device_id={"tp": to},
            device_id_type=MESH,
        )

    def spread_arrival(i, src):
        return spread(i, src, across)

    spreads = [spread(0, tp, across), spread(1, tp, beside), spread(2, across, beside)]
    spreads[0].start()
    spreads[1].start()

    groups = 4
    chips = n_z // groups
    per = 2 * chips
    half_rows = per * cap

    def swap(o):
        return pltpu.make_async_remote_copy(
            src_ref=in_buf.at[pl.ds(2 * o, 2)],
            dst_ref=peer_buf.at[pl.ds(2 * o, 2)],
            send_sem=swap_send.at[o],
            recv_sem=swap_recv.at[o],
            device_id={"tp": across},
            device_id_type=MESH,
        )

    def pass_on(o):
        if o in near or o == last:
            token_arrival(o, 1 - core).wait_recv()
        else:
            for k in range(2):
                token_arrival(o, k).wait_recv()
        swap(o).start()

    def pass_all(first, end):
        for o in range(first, end):
            pass_on(o)

    pass_on(last)
    for side in range(2):
        arrived = [along(side, 0, meta, meta_in.at[side]), along(side, 1, xin, stream.at[side])]
        for copy in arrived:
            copy.wait_recv()
        first = (2 * z, (2 * (z + 1 + half) + 1) % n_ep)[side]
        rows_of = pick(stream.at[side], meta_in[side], first, blocks)
        for c in range(0, width, step):
            relay[side, :, :, c : c + step] = rows_of(c)
        for copy in relays[side]:
            copy.start()
        siblings[1 + side].start()
        in_buf[2 * near[side] + core] = relay[side, here_at[side] + core]

    def partial_copy(o):
        mine = pl.ds(o % chips * 2 * cap, 2 * cap)
        return pltpu.make_async_remote_copy(
            src_ref=part_out.at[o // chips, mine],
            dst_ref=part_back.at[o // chips, mine],
            send_sem=back_send.at[o],
            recv_sem=back_recv.at[o],
            device_id={"tp": across},
            device_id_type=MESH,
        )

    def hide(g):
        @pl.loop(g * chips, (g + 1) * chips)
        def _(o):
            swap(o).wait_recv()

        mine = pl.ds(g * per, per)
        x = jnp.concatenate(
            [
                peer_buf[mine].reshape(half_rows, width),
                in_buf[mine].reshape(half_rows, width),
            ],
            axis=0,
        )
        for s in range(2):
            gate_in = dot(x, wg[s])
            hidden[g, s] = (gate_in / (1.0 + jnp.exp(-gate_in)) * dot(x, wu[s])).astype(BF16)

    def lower(g):
        for c in range(0, width, step):
            total = dot(hidden[g, 0], wd[0, :, c : c + step]).astype(BF16).astype(F32)
            total = total + dot(hidden[g, 1], wd[1, :, c : c + step]).astype(BF16).astype(F32)
            part_out[g, :, c : c + step] = total[:half_rows].astype(BF16)
            acc[g, :, c : c + step] = total[half_rows:]
        for o in range(g * chips, (g + 1) * chips):
            partial_copy(o).start()

    def result_copy(o, k):
        to = 2 * ((z + n_z - offset(o, n_z)) % n_z) + k
        return pltpu.make_async_remote_copy(
            src_ref=res_buf.at[2 * o + k],
            dst_ref=ret_buf.at[ep],
            send_sem=ret_send.at[2 * o + k],
            recv_sem=ret_recv.at[2 * o + core],
            device_id={"ep": to},
            device_id_type=MESH,
        )

    def result_arrival(o, k):
        sender = 2 * ((z + offset(o, n_z)) % n_z) + k
        return pltpu.make_async_remote_copy(
            src_ref=res_buf.at[2 * o + k],
            dst_ref=ret_buf.at[sender],
            send_sem=ret_send.at[2 * o + k],
            recv_sem=ret_recv.at[2 * o + k],
            device_id={"ep": 2 * z + 1 - core},
            device_id_type=MESH,
        )

    sibling_back = pltpu.make_async_remote_copy(
        src_ref=res_buf.at[2 * last + 1 - core],
        dst_ref=ret_buf.at[ep],
        send_sem=ret_send.at[2 * last + 1 - core],
        recv_sem=ret_recv.at[2 * last + core],
        device_id={"ep": 2 * z + 1 - core},
        device_id_type=MESH,
    )

    def answer(g):
        for o in range(g * chips, (g + 1) * chips):
            partial_copy(o).wait_recv()
            mine = pl.ds(o % chips * 2 * cap, 2 * cap)
            res_buf[pl.ds(2 * o, 2)] = (
                (acc[g, mine] + part_back[g, mine].astype(F32)).astype(BF16).reshape(2, cap, width)
            )
            for k in range(2):
                if o < last:
                    result_copy(o, k).start()

        if g == groups - 1:
            sibling_back.start()
            ret_buf[ep] = res_buf[2 * last + core]

    pass_all(0, 2 * chips)

    @pl.when(tp != n_tp - 1)
    def _():
        tail_copy(0).wait_recv()

    edge_out[...] = dot(tail[...], inw_v[...]).astype(BF16)
    halo = pltpu.make_async_remote_copy(
        src_ref=edge_out,
        dst_ref=edge_in,
        send_sem=halo_send,
        recv_sem=halo_recv,
        device_id={"ep": (ep + 1) % n_ep},
        device_id_type=MESH,
    )
    halo.start()
    spread_arrival(0, across).wait_recv()
    spreads[2].start()

    pass_all(2 * chips, 3 * chips)
    for i in range(8, 11):
        loads[i].wait()
    for copy in shard_copies[:2]:
        copy.wait_recv()
    hide(0)
    hide(1)
    shard_copies[2].wait_recv()
    lower(0)
    lower(1)
    answer(0)
    pass_all(3 * chips, last)
    hide(2)
    lower(2)
    answer(1)
    hide(3)
    lower(3)
    answer(2)

    for i in (3, 5, 11, 12):
        loads[i].wait()
    ext[0] = jnp.zeros((rows, ext.shape[2]), BF16)
    for i, src in enumerate((across, beside, opposite)):
        if i:
            spread_arrival(i, src).wait_recv()
        ext[src + 1] = dot(normed[src], inw_v[...]).astype(BF16)
    ext[tp + 1] = dot(normed[tp], inw_v[...]).astype(BF16)
    window = jnp.left_shift(jnp.int32(2), tp)
    lag = lax.broadcasted_iota(jnp.int32, (rows, rows), 0) - lax.broadcasted_iota(
        jnp.int32, (rows, rows), 1
    )
    band = jnp.where((lag >= 0) & (lag < window), 1.0, 0.0).astype(BF16)
    band_before = jnp.where(lag + rows < window, 1.0, 0.0).astype(BF16)
    place_in = lax.broadcasted_iota(jnp.int32, (rows, 1), 0) + 1
    halo.wait_recv()
    ext[0, edge, :] = jnp.where(ep == 0, 0.0, edge_in[...].astype(F32)).astype(BF16)

    def sums(i, src, to):
        return pltpu.make_async_remote_copy(
            src_ref=part_buf.at[src],
            dst_ref=part_in.at[i],
            send_sem=rs_send.at[i],
            recv_sem=rs_recv.at[i],
            device_id={"tp": to},
            device_id_type=MESH,
        )

    parts = [sums(0, beside, beside), sums(1, opposite, beside), sums(2, across, across)]
    for i, m in ((1, opposite), (0, beside), (2, across), (3, tp)):
        here = ext[m + 1]
        total = dot(band, here) + dot(band_before, ext[m])
        counts = jnp.minimum(place_in + (ep * n_tp + m) * rows, window).astype(F32)
        pooled = (total / counts - here.astype(F32)).astype(BF16)
        grouped = (dot(pooled, gw_v[...]) * scale[...].astype(F32)[None]).astype(BF16)
        for c in range(0, width, step):
            part_buf[m, :, c : c + step] = dot(grouped, ow_v[:, c : c + step]).astype(BF16)
        if i < 2:
            parts[i].start()

    answer(3)

    parts[1].wait_recv()
    part_buf[across] = (part_buf[across].astype(F32) + part_in[1].astype(F32)).astype(BF16)
    parts[2].start()
    parts[0].wait_recv()
    parts[2].wait_recv()
    mixed_out[...] = (
        part_buf[tp].astype(F32) + part_in[0].astype(F32) + part_in[2].astype(F32)
    ).astype(BF16)

    ids = jnp.transpose(ids_t[...])
    shares = jnp.transpose(shares_t[...])
    lanes = lax.broadcasted_iota(jnp.int32, (rows, n_ep), 1)
    mine = [ids[:, k : k + 1] == lanes for k in range(2)]
    named_rows = jnp.where(mine[0] | mine[1], 1.0, 0.0).astype(BF16)
    later = jnp.where(lag > 0, 1.0, 0.0).astype(BF16)
    before_rows = dot(later, named_rows)
    slots = lax.broadcasted_iota(jnp.int32, (rows, n_slots), 1)
    picks = []
    for k in range(2):
        target = ids[:, k : k + 1] * cap + jnp.sum(
            jnp.where(mine[k], before_rows, 0.0), axis=1, keepdims=True
        ).astype(jnp.int32)
        picks.append(jnp.where(slots == target, 1.0, 0.0).astype(BF16))
    weight = shares / jnp.sum(shares, axis=1, keepdims=True)

    def await_results(o):
        for k in range(2):
            result_arrival(o, k).wait_recv()

    each(0, last, await_results)
    pltpu.make_async_remote_copy(
        src_ref=res_buf.at[2 * last + 1 - core],
        dst_ref=ret_buf.at[2 * z + 1 - core],
        send_sem=ret_send.at[2 * last + 1 - core],
        recv_sem=ret_recv.at[2 * last + 1 - core],
        device_id={"ep": 2 * z + 1 - core},
        device_id_type=MESH,
    ).wait_recv()

    for c in range(0, width, step):
        back = ret_buf[:, :, c : c + step].reshape(n_slots, step)
        mix = dot(picks[0], back) * weight[:, 0:1] + dot(picks[1], back) * weight[:, 1:2]
        expert_out[:, c : c + step] = mix.astype(BF16)

    for copy in (*shard_copies, *streams, *relays[0], *relays[1], *siblings, sibling_back):
        copy.wait_send()

    def await_sent(o):
        for k in range(2):
            result_copy(o, k).wait_send()

    each(0, last, await_sent)

    @pl.loop(0, n_z)
    def _(o):
        swap(o).wait_send()

    for o in range(n_z):
        partial_copy(o).wait_send()

    for copy in (*spreads, *parts):
        copy.wait_send()
    halo.wait_send()

    @pl.when(tp == n_tp - 1)
    def _():
        for r in range(1, n_tp):
            tail_copy(r).wait_send()


def solution(mesh):
    n_ep, n_tp = mesh.shape["ep"], mesh.shape["tp"]

    def local(
        mixer_tokens, mixer_gain, in_weight, group_weight, channel_scale, out_weight,
        expert_tokens, expert_gain, route_ids, route_weights, gate_weight, up_weight, down_weight,
    ):
        rows, width = expert_tokens.shape
        cap = 4 * rows // n_ep
        gw = in_weight.shape[1]
        ff = gate_weight.shape[2]
        vmem = pl.BlockSpec(memory_space=pltpu.VMEM)
        hbm = pl.BlockSpec(memory_space=pl.ANY)
        slots = n_ep * cap
        V = pltpu.VMEM
        dma = pltpu.SemaphoreType.DMA
        out = jax.ShapeDtypeStruct((rows, width), BF16)
        return pl.pallas_call(
            functools.partial(kernel, n_ep, n_tp, cap),
            out_shape=(out, out),
            in_specs=[hbm] * 13,
            out_specs=(vmem, vmem),
            scratch_shapes=[
                V((rows, width), BF16),
                V((width,), BF16),
                V((width,), BF16),
                V((gw,), BF16),
                V((2, rows), jnp.int32),
                V((2, rows), F32),
                V((rows, width), BF16),
                V((2, rows), F32),
                V((2, cap, width), BF16),
                V((2, rows, width), BF16),
                V((2, 2, rows), F32),
                V((2, n_ep // 2 - 1, cap, width), BF16),
                V((n_ep, cap, width), BF16),
                V((n_ep, cap, width), BF16),
                V((n_ep, cap, width), BF16),
                V((n_ep, cap, width), BF16),
                V((4, 2, slots // 2, ff), BF16),
                V((4, slots // 4, width), F32),
                V((4, slots // 4, width), BF16),
                V((4, slots // 4, width), BF16),
                V((2, width, ff), BF16),
                V((2, width, ff), BF16),
                V((2, ff, width), BF16),
                V((rows, width), BF16),
                V((n_tp, rows, width), BF16),
                V((WINDOW_MAX, width), BF16),
                V((WINDOW_MAX, gw), BF16),
                V((WINDOW_MAX, gw), BF16),
                V((width, gw), BF16),
                V((gw, gw), BF16),
                V((gw, width), BF16),
                V((n_tp + 1, rows, gw), BF16),
                V((n_tp, rows, width), BF16),
                V((n_tp - 1, rows, width), BF16),
                dma((13,)),
                dma((4,)),
                dma((4,)),
                dma((n_ep,)),
                dma((n_ep,)),
                dma((n_ep // 2,)),
                dma((n_ep // 2,)),
                dma((n_ep // 2,)),
                dma((n_ep // 2,)),
                dma((n_ep,)),
                dma((n_ep,)),
                dma((3,)),
                dma((3,)),
                dma((n_tp,)),
                dma((n_tp,)),
                dma((n_tp,)),
                dma,
                dma,
                dma,
                dma((n_tp,)),
                dma((n_tp,)),
            ],
            compiler_params=pltpu.CompilerParams(
                collective_id=0, has_side_effects=True, vmem_limit_bytes=52 * 1024 * 1024
            ),
        )(
            *(
                pltpu.with_memory_space_constraint(a, pltpu.HBM)
                for a in (
                    mixer_tokens, mixer_gain, in_weight, group_weight, channel_scale, out_weight,
                    expert_tokens, expert_gain, route_ids.T, route_weights.T,
                    gate_weight, up_weight, down_weight,
                )
            )
        )

    block = P(("grp", "ep", "tp"), None)
    placed = (
        block, P(), P(None, "tp"), P("tp", None, None), P("tp"), P("tp", None),
        block, P(), block, block, P("ep", None, "tp"), P("ep", None, "tp"), P("ep", "tp", None),
    )
    return jax.shard_map(
        local, mesh=mesh, in_specs=placed, out_specs=(block, block), check_vma=False
    )
```

```python
import functools

import jax
import jax.numpy as jnp
from jax import lax
from jax.experimental import pallas as pl
from jax.experimental.pallas import tpu as pltpu
from jax.sharding import PartitionSpec as P

MESH = pl.DeviceIdType.MESH
F32 = jnp.float32
BF16 = jnp.bfloat16
WINDOW_MAX = 16


def dot(a, b):
    return jnp.dot(a, b, preferred_element_type=F32)


def rms_rows(rows, gain):
    values = rows.astype(F32)
    scaled = values * lax.rsqrt(jnp.mean(values * values, axis=-1, keepdims=True) + 1e-06)
    return (scaled * gain.astype(F32)[None]).astype(BF16)


def offset(j, n):
    if not isinstance(j, int) or j < n - 4:
        pair, i = j // 4, j % 4
        hops = (1 - i // 2) * (n // 2 - 1 - pair) + (i // 2) * (1 + pair)
        return (n + (1 - 2 * (i % 2)) * hops) % n
    return (n // 2, n // 4, 3 * n // 4, 0)[j - n + 4]


def kernel(
    n_ep, n_tp, cap,
    mtok, mgain_h, inw, gw, scale_h, ow, etok_h, egain_h, ids_h, shares_h, gate, up, down,
    mixed_out, expert_out,
    etok, egain, mgain, scale, ids_t, shares_t,
    xin, meta, own_buf, stream, meta_in, relay, in_buf, peer_buf, res_buf, back, own_back, sums_out, home, hidden, acc, part_out, part_back, wg, wu, wd,
    mrows, normed, tail, edge_out, edge_in, inw_v, gw_v, ow_v, ext, part_buf, part_in,
    load_sem, stream_send, stream_recv, tok_send, tok_recv, swap_send, swap_recv, back_send, back_recv,
    ret_send, ret_recv, home_send, home_recv, w_send, w_recv,
    ag_send, ag_recv, tail_send, tail_recv, halo_send, halo_recv, rs_send, rs_recv,
):
    ep = lax.axis_index("ep")
    tp = lax.axis_index("tp")
    rows, width = mtok.shape
    n_slots = n_ep * cap
    beside, across = tp + 1 - 2 * (tp % 2), n_tp - 1 - tp
    opposite = n_tp - 1 - beside
    n_z = n_ep // 2
    z, core = ep // 2, ep % 2

    barrier = pltpu.get_barrier_semaphore()

    @pl.loop(1, n_ep)
    def _(r):
        pl.semaphore_signal(
            barrier, inc=1, device_id={"ep": (ep + r) % n_ep}, device_id_type=MESH
        )

    for r in range(1, n_tp):
        pl.semaphore_signal(
            barrier, inc=1, device_id={"tp": (tp + r) % n_tp}, device_id_type=MESH
        )

    loads = [
        pltpu.make_async_copy(src, dst, load_sem.at[i])
        for i, (src, dst) in enumerate(
            [
                (etok_h, etok),
                (egain_h, egain),
                (ids_h, ids_t),
                (shares_h, shares_t),
                (mgain_h, mgain),
                (scale_h, scale),
                (mtok, mrows),
                (inw, inw_v),
                (gate.at[0], wg.at[0]),
                (up.at[0], wu.at[0]),
                (down.at[0], wd.at[0]),
                (gw.at[0], gw_v),
                (ow, ow_v),
            ]
        )
    ]
    for load in loads:
        load.start()
    for i in range(4):
        loads[i].wait()

    def weights(i, src, dst):
        return pltpu.make_async_remote_copy(
            src_ref=src,
            dst_ref=dst,
            send_sem=w_send.at[i],
            recv_sem=w_recv.at[i],
            device_id={"tp": beside},
            device_id_type=MESH,
        )

    shard_copies = [
        weights(0, gate.at[0], wg.at[1]),
        weights(1, up.at[0], wu.at[1]),
        weights(2, down.at[0], wd.at[1]),
    ]

    xin[...] = rms_rows(etok[...], egain[...])
    experts = lax.broadcasted_iota(jnp.int32, (n_ep, rows), 0)
    firsts = [ids_t[k : k + 1, :] == experts for k in range(2)]
    named = jnp.where(firsts[0] | firsts[1], 1.0, 0.0).astype(BF16)
    earlier = jnp.where(
        lax.broadcasted_iota(jnp.int32, (rows, rows), 0)
        < lax.broadcasted_iota(jnp.int32, (rows, rows), 1),
        1.0,
        0.0,
    ).astype(BF16)
    before = dot(named, earlier)
    targets_t = [
        ids_t[k : k + 1, :] * cap
        + jnp.sum(jnp.where(firsts[k], before, 0.0), axis=0, keepdims=True).astype(jnp.int32)
        for k in range(2)
    ]
    for k in range(2):
        meta[k : k + 1, :] = targets_t[k].astype(F32)
    weight = shares_t[...]
    meta[2:4, :] = weight / jnp.sum(weight, axis=0, keepdims=True)

    def pick(tokens, targets, first, count):
        place = lax.broadcasted_iota(jnp.int32, (count * cap, rows), 0) + first * cap
        place = jnp.where(place >= n_slots, place - n_slots, place).astype(F32)
        chosen = jnp.where(
            (place == targets[0:1, :]) | (place == targets[1:2, :]), 1.0, 0.0
        ).astype(BF16)
        return lambda c: dot(chosen, tokens[:, c : c + step]).astype(BF16).reshape(count, cap, step)

    step = min(512, width)
    own = pick(xin, meta[...], 2 * z, 2)
    for c in range(0, width, step):
        own_buf[:, :, c : c + step] = own(c)
    last = n_z - 1
    in_buf[2 * last + core] = own_buf[core]
    order = [offset(o, n_z) for o in range(n_z)]
    ahead = [(z + 1) % n_z, (z + n_z - 1) % n_z]

    def along(side, i, src, dst):
        return pltpu.make_async_remote_copy(
            src_ref=src,
            dst_ref=dst,
            send_sem=stream_send.at[2 * side + i],
            recv_sem=stream_recv.at[2 * side + i],
            device_id={"ep": 2 * ahead[side] + core},
            device_id_type=MESH,
        )

    streams = [
        copy
        for side in range(2)
        for copy in (
            along(side, 0, meta, meta_in.at[side]),
            along(side, 1, xin, stream.at[side]),
        )
    ]

    pl.semaphore_wait(barrier, n_ep - 1 + n_tp - 1)

    for copy in streams:
        copy.start()

    def to_sibling(o, src):
        return pltpu.make_async_remote_copy(
            src_ref=src,
            dst_ref=in_buf.at[2 * o + core],
            send_sem=tok_send.at[2 * o + 1 - core],
            recv_sem=tok_recv.at[2 * o + core],
            device_id={"ep": 2 * z + 1 - core},
            device_id_type=MESH,
        )

    def relayed(o, k, side, block):
        to = 2 * ((z + order[o] + n_z + (-1, 1)[side]) % n_z) + k
        return pltpu.make_async_remote_copy(
            src_ref=relay.at[side, block],
            dst_ref=in_buf.at[2 * o + core],
            send_sem=tok_send.at[2 * o + k],
            recv_sem=tok_recv.at[2 * o + core],
            device_id={"ep": to},
            device_id_type=MESH,
        )

    def token_arrival(o, k):
        return pltpu.make_async_remote_copy(
            src_ref=in_buf.at[2 * o + k],
            dst_ref=in_buf.at[2 * o + k],
            send_sem=tok_send.at[2 * o + k],
            recv_sem=tok_recv.at[2 * o + k],
            device_id={"ep": 2 * z + 1 - core},
            device_id_type=MESH,
        )

    half = n_z // 2
    blocks = n_z - 1
    near = [order.index(1), order.index(n_z - 1)]
    here_at = [0, blocks - 2]
    firsts_at = [2 * z, (2 * (z + 1 + half) + 1) % n_ep]
    relays = [[], []]
    for o in range(last):
        d = order[o]
        for k in range(2):
            if 2 <= d < half or (d == half and k == 0):
                relays[0].append(relayed(o, k, 0, 2 * (d - 1) + k))
            elif half < d <= n_z - 2 or d == half:
                relays[1].append(relayed(o, k, 1, 2 * (half - (n_z - d)) + k - 1))
    siblings = [to_sibling(last, own_buf.at[1 - core])] + [
        to_sibling(near[side], relay.at[side, here_at[side] + 1 - core]) for side in range(2)
    ]
    siblings[0].start()
    shard_copies[0].start()

    loads[4].wait()
    loads[6].wait()
    normed[tp] = rms_rows(mrows[...], mgain[...])

    edge = pl.ds(rows - WINDOW_MAX, WINDOW_MAX)

    def tail_copy(r):
        return pltpu.make_async_remote_copy(
            src_ref=normed.at[n_tp - 1, edge],
            dst_ref=tail,
            send_sem=tail_send.at[r],
            recv_sem=tail_recv,
            device_id={"tp": (tp + r) % n_tp},
            device_id_type=MESH,
        )

    loads[7].wait()

    @pl.when(tp == n_tp - 1)
    def _():
        for r in (2, 1, 3):
            tail_copy(r).start()
        tail[...] = normed[n_tp - 1, edge]

    for copy in shard_copies[1:]:
        copy.start()

    def spread(i, src, to):
        return pltpu.make_async_remote_copy(
            src_ref=normed.at[src],
            dst_ref=normed.at[src],
            send_sem=ag_send.at[i],
            recv_sem=ag_recv.at[i],
            device_id={"tp": to},
            device_id_type=MESH,
        )

    def spread_arrival(i, src):
        return spread(i, src, across)

    spreads = [spread(0, tp, across), spread(1, tp, beside), spread(2, across, beside)]
    spreads[0].start()
    spreads[1].start()

    groups = 4
    chips = n_z // groups
    per = 2 * chips
    half_rows = per * cap

    def swap(o):
        return pltpu.make_async_remote_copy(
            src_ref=in_buf.at[pl.ds(2 * o, 2)],
            dst_ref=peer_buf.at[pl.ds(2 * o, 2)],
            send_sem=swap_send.at[o],
            recv_sem=swap_recv.at[o],
            device_id={"tp": across},
            device_id_type=MESH,
        )

    def pass_on(o):
        if o in near or o == last:
            token_arrival(o, 1 - core).wait_recv()
        else:
            for k in range(2):
                token_arrival(o, k).wait_recv()
        swap(o).start()

    def pass_all(first, end):
        for o in range(first, end):
            pass_on(o)

    pass_on(last)
    for side in range(2):
        arrived = [along(side, 0, meta, meta_in.at[side]), along(side, 1, xin, stream.at[side])]
        for copy in arrived:
            copy.wait_recv()
        rows_of = pick(stream.at[side], meta_in[side], firsts_at[side], blocks)
        for c in range(0, width, step):
            relay[side, :, :, c : c + step] = rows_of(c)
        for copy in relays[side]:
            copy.start()
        siblings[1 + side].start()
        in_buf[2 * near[side] + core] = relay[side, here_at[side] + core]

    def partial_copy(o):
        mine = pl.ds(o % chips * 2 * cap, 2 * cap)
        return pltpu.make_async_remote_copy(
            src_ref=part_out.at[o // chips, mine],
            dst_ref=part_back.at[o // chips, mine],
            send_sem=back_send.at[o],
            recv_sem=back_recv.at[o],
            device_id={"tp": across},
            device_id_type=MESH,
        )

    def hide(g):
        @pl.loop(g * chips, (g + 1) * chips)
        def _(o):
            swap(o).wait_recv()

        mine = pl.ds(g * per, per)
        x = jnp.concatenate(
            [
                peer_buf[mine].reshape(half_rows, width),
                in_buf[mine].reshape(half_rows, width),
            ],
            axis=0,
        )
        for s in range(2):
            gate_in = dot(x, wg[s])
            hidden[g, s] = (gate_in / (1.0 + jnp.exp(-gate_in)) * dot(x, wu[s])).astype(BF16)

    def lower(g):
        for c in range(0, width, step):
            total = dot(hidden[g, 0], wd[0, :, c : c + step]).astype(BF16).astype(F32)
            total = total + dot(hidden[g, 1], wd[1, :, c : c + step]).astype(BF16).astype(F32)
            part_out[g, :, c : c + step] = total[:half_rows].astype(BF16)
            acc[g, :, c : c + step] = total[half_rows:]
        for o in range(g * chips, (g + 1) * chips):
            partial_copy(o).start()

    def result_copy(o, k):
        d = order[o]
        origin = z + n_z - d
        if d == half:
            side, block, to = core, (1 - core) * (blocks - 1), origin + 1 - 2 * core
        elif d < half:
            side, block, to = 0, 2 * (d - 1) + core, origin + 1
        else:
            side, block, to = 1, 2 * (half - (n_z - d)) + core - 1, origin - 1
        return pltpu.make_async_remote_copy(
            src_ref=res_buf.at[2 * o + k],
            dst_ref=back.at[side, block],
            send_sem=ret_send.at[2 * o + k],
            recv_sem=ret_recv.at[side * blocks + block],
            device_id={"ep": 2 * (to % n_z) + k},
            device_id_type=MESH,
        )

    def result_to_sibling(o, dst, sem):
        return pltpu.make_async_remote_copy(
            src_ref=res_buf.at[2 * o + 1 - core],
            dst_ref=dst,
            send_sem=ret_send.at[2 * o + 1 - core],
            recv_sem=ret_recv.at[sem],
            device_id={"ep": 2 * z + 1 - core},
            device_id_type=MESH,
        )

    def result_arrival(dst, sem):
        return result_to_sibling(last, dst, sem)

    results = {
        o: [result_copy(o, k) for k in range(2)] for o in range(last) if o not in near
    }
    for side in range(2):
        block = here_at[side] + core
        results[near[side]] = [
            result_to_sibling(near[side], back.at[side, block], side * blocks + block)
        ]
    results[last] = [result_to_sibling(last, own_back.at[core], 2 * blocks + core)]

    def answer(g):
        for o in range(g * chips, (g + 1) * chips):
            partial_copy(o).wait_recv()
            mine = pl.ds(o % chips * 2 * cap, 2 * cap)
            res_buf[pl.ds(2 * o, 2)] = (
                (acc[g, mine] + part_back[g, mine].astype(F32)).astype(BF16).reshape(2, cap, width)
            )
            for copy in results[o]:
                copy.start()
            if o in near:
                side = near.index(o)
                back[side, here_at[side] + core] = res_buf[2 * o + core]

        if g == groups - 1:
            own_back[core] = res_buf[2 * last + core]

    pass_all(0, 2 * chips)

    @pl.when(tp != n_tp - 1)
    def _():
        tail_copy(0).wait_recv()

    edge_out[...] = dot(tail[...], inw_v[...]).astype(BF16)
    halo = pltpu.make_async_remote_copy(
        src_ref=edge_out,
        dst_ref=edge_in,
        send_sem=halo_send,
        recv_sem=halo_recv,
        device_id={"ep": (ep + 1) % n_ep},
        device_id_type=MESH,
    )
    halo.start()
    spread_arrival(0, across).wait_recv()
    spreads[2].start()

    pass_all(2 * chips, 3 * chips)
    for i in range(8, 11):
        loads[i].wait()
    for copy in shard_copies[:2]:
        copy.wait_recv()
    hide(0)
    hide(1)
    shard_copies[2].wait_recv()
    lower(0)
    lower(1)
    answer(0)
    pass_all(3 * chips, last)
    hide(2)
    lower(2)
    answer(1)
    hide(3)
    lower(3)
    answer(2)

    for i in (5, 11, 12):
        loads[i].wait()
    ext[0] = jnp.zeros((rows, ext.shape[2]), BF16)
    for i, src in enumerate((across, beside, opposite)):
        if i:
            spread_arrival(i, src).wait_recv()
        ext[src + 1] = dot(normed[src], inw_v[...]).astype(BF16)
    ext[tp + 1] = dot(normed[tp], inw_v[...]).astype(BF16)
    window = jnp.left_shift(jnp.int32(2), tp)
    lag = lax.broadcasted_iota(jnp.int32, (rows, rows), 0) - lax.broadcasted_iota(
        jnp.int32, (rows, rows), 1
    )
    band = jnp.where((lag >= 0) & (lag < window), 1.0, 0.0).astype(BF16)
    band_before = jnp.where(lag + rows < window, 1.0, 0.0).astype(BF16)
    place_in = lax.broadcasted_iota(jnp.int32, (rows, 1), 0) + 1
    halo.wait_recv()
    ext[0, edge, :] = jnp.where(ep == 0, 0.0, edge_in[...].astype(F32)).astype(BF16)

    def sums(i, src, to):
        return pltpu.make_async_remote_copy(
            src_ref=part_buf.at[src],
            dst_ref=part_in.at[i],
            send_sem=rs_send.at[i],
            recv_sem=rs_recv.at[i],
            device_id={"tp": to},
            device_id_type=MESH,
        )

    parts = [sums(0, beside, beside), sums(1, opposite, beside), sums(2, across, across)]
    for i, m in ((1, opposite), (0, beside), (2, across), (3, tp)):
        here = ext[m + 1]
        total = dot(band, here) + dot(band_before, ext[m])
        counts = jnp.minimum(place_in + (ep * n_tp + m) * rows, window).astype(F32)
        pooled = (total / counts - here.astype(F32)).astype(BF16)
        grouped = (dot(pooled, gw_v[...]) * scale[...].astype(F32)[None]).astype(BF16)
        for c in range(0, width, step):
            part_buf[m, :, c : c + step] = dot(grouped, ow_v[:, c : c + step]).astype(BF16)
        if i < 2:
            parts[i].start()

    answer(3)

    parts[1].wait_recv()
    part_buf[across] = (part_buf[across].astype(F32) + part_in[1].astype(F32)).astype(BF16)
    parts[2].start()
    parts[0].wait_recv()
    parts[2].wait_recv()
    mixed_out[...] = (
        part_buf[tp].astype(F32) + part_in[0].astype(F32) + part_in[2].astype(F32)
    ).astype(BF16)

    def mixed_rows(told, first, count):
        told = jnp.transpose(told)
        place = lax.broadcasted_iota(jnp.int32, (rows, count * cap), 1) + first * cap
        place = jnp.where(place >= n_slots, place - n_slots, place).astype(F32)
        picks = [jnp.where(place == told[:, k : k + 1], 1.0, 0.0).astype(BF16) for k in range(2)]
        return lambda found: (
            dot(picks[0], found) * told[:, 2:3] + dot(picks[1], found) * told[:, 3:4]
        )

    def homeward(side, h):
        return pltpu.make_async_remote_copy(
            src_ref=sums_out.at[side, h],
            dst_ref=home.at[side, h],
            send_sem=home_send.at[2 * side + h],
            recv_sem=home_recv.at[2 * side + h],
            device_id={"ep": 2 * ahead[1 - side] + core},
            device_id_type=MESH,
        )

    wide = width // 2
    part_step = min(step, wide)
    for side in range(2):
        for block in range(blocks):
            if block not in (here_at[side], here_at[side] + 1):
                result_arrival(back.at[side, block], side * blocks + block).wait_recv()
        block = here_at[side] + 1 - core
        result_arrival(back.at[side, block], side * blocks + block).wait_recv()
        weigh = mixed_rows(meta_in[side], firsts_at[side], blocks)
        for h in range(2):
            for c in range(0, wide, part_step):
                at = h * wide + c
                found = back[side, :, :, at : at + part_step].reshape(blocks * cap, part_step)
                sums_out[side, h, :, c : c + part_step] = weigh(found).astype(BF16)
            homeward(side, h).start()

    result_arrival(own_back.at[1 - core], 2 * blocks + 1 - core).wait_recv()
    weigh = mixed_rows(meta[...], 2 * z, 2)
    for h in range(2):
        for side in range(2):
            homeward(side, h).wait_recv()
        for c in range(0, wide, part_step):
            at = h * wide + c
            total = weigh(own_back[:, :, at : at + part_step].reshape(2 * cap, part_step))
            for side in range(2):
                total = total + home[side, h, :, c : c + part_step].astype(F32)
            expert_out[:, at : at + part_step] = total.astype(BF16)

    for copy in (*shard_copies, *streams, *relays[0], *relays[1], *siblings):
        copy.wait_send()

    for o in range(n_z):
        for copy in results[o]:
            copy.wait_send()
    for side in range(2):
        for h in range(2):
            homeward(side, h).wait_send()

    @pl.loop(0, n_z)
    def _(o):
        swap(o).wait_send()

    for o in range(n_z):
        partial_copy(o).wait_send()

    for copy in (*spreads, *parts):
        copy.wait_send()
    halo.wait_send()

    @pl.when(tp == n_tp - 1)
    def _():
        for r in range(1, n_tp):
            tail_copy(r).wait_send()


def solution(mesh):
    n_ep, n_tp = mesh.shape["ep"], mesh.shape["tp"]

    def local(
        mixer_tokens, mixer_gain, in_weight, group_weight, channel_scale, out_weight,
        expert_tokens, expert_gain, route_ids, route_weights, gate_weight, up_weight, down_weight,
    ):
        rows, width = expert_tokens.shape
        cap = 4 * rows // n_ep
        gw = in_weight.shape[1]
        ff = gate_weight.shape[2]
        vmem = pl.BlockSpec(memory_space=pltpu.VMEM)
        hbm = pl.BlockSpec(memory_space=pl.ANY)
        slots = n_ep * cap
        V = pltpu.VMEM
        dma = pltpu.SemaphoreType.DMA
        out = jax.ShapeDtypeStruct((rows, width), BF16)
        return pl.pallas_call(
            functools.partial(kernel, n_ep, n_tp, cap),
            out_shape=(out, out),
            in_specs=[hbm] * 13,
            out_specs=(vmem, vmem),
            scratch_shapes=[
                V((rows, width), BF16),
                V((width,), BF16),
                V((width,), BF16),
                V((gw,), BF16),
                V((2, rows), jnp.int32),
                V((2, rows), F32),
                V((rows, width), BF16),
                V((4, rows), F32),
                V((2, cap, width), BF16),
                V((2, rows, width), BF16),
                V((2, 4, rows), F32),
                V((2, n_ep // 2 - 1, cap, width), BF16),
                V((n_ep, cap, width), BF16),
                V((n_ep, cap, width), BF16),
                V((n_ep, cap, width), BF16),
                V((2, n_ep // 2 - 1, cap, width), BF16),
                V((2, cap, width), BF16),
                V((2, 2, rows, width // 2), BF16),
                V((2, 2, rows, width // 2), BF16),
                V((4, 2, slots // 2, ff), BF16),
                V((4, slots // 4, width), F32),
                V((4, slots // 4, width), BF16),
                V((4, slots // 4, width), BF16),
                V((2, width, ff), BF16),
                V((2, width, ff), BF16),
                V((2, ff, width), BF16),
                V((rows, width), BF16),
                V((n_tp, rows, width), BF16),
                V((WINDOW_MAX, width), BF16),
                V((WINDOW_MAX, gw), BF16),
                V((WINDOW_MAX, gw), BF16),
                V((width, gw), BF16),
                V((gw, gw), BF16),
                V((gw, width), BF16),
                V((n_tp + 1, rows, gw), BF16),
                V((n_tp, rows, width), BF16),
                V((n_tp - 1, rows, width), BF16),
                dma((13,)),
                dma((4,)),
                dma((4,)),
                dma((n_ep,)),
                dma((n_ep,)),
                dma((n_ep // 2,)),
                dma((n_ep // 2,)),
                dma((n_ep // 2,)),
                dma((n_ep // 2,)),
                dma((n_ep,)),
                dma((n_ep,)),
                dma((4,)),
                dma((4,)),
                dma((3,)),
                dma((3,)),
                dma((n_tp,)),
                dma((n_tp,)),
                dma((n_tp,)),
                dma,
                dma,
                dma,
                dma((n_tp,)),
                dma((n_tp,)),
            ],
            compiler_params=pltpu.CompilerParams(
                collective_id=0, has_side_effects=True, vmem_limit_bytes=52 * 1024 * 1024
            ),
        )(
            *(
                pltpu.with_memory_space_constraint(a, pltpu.HBM)
                for a in (
                    mixer_tokens, mixer_gain, in_weight, group_weight, channel_scale, out_weight,
                    expert_tokens, expert_gain, route_ids.T, route_weights.T,
                    gate_weight, up_weight, down_weight,
                )
            )
        )

    block = P(("grp", "ep", "tp"), None)
    placed = (
        block, P(), P(None, "tp"), P("tp", None, None), P("tp"), P("tp", None),
        block, P(), block, block, P("ep", None, "tp"), P("ep", None, "tp"), P("ep", "tp", None),
    )
    return jax.shard_map(
        local, mesh=mesh, in_specs=placed, out_specs=(block, block), check_vma=False
    )
```
